512 devices in a mesh: ep: 128 (over z, y, core), tp: 4 (over x).
Axes of the slice: x: 4, y: 8, z: 8, core: 2. Of those that a mesh axis runs over, the one named last changes fastest.
Arguments:
- tokens: bfloat16 [256, 2048], P('ep'), may hold values from -6 to 6
- state_c: float32 [256, 8, 128, 256], P('ep', 'tp'), may hold values from -0.8 to 0.8
- state_n: float32 [256, 8, 128], P('ep', 'tp'), may hold values from -0.8 to 0.8
- state_m: float32 [256, 8], P('ep', 'tp'), may hold values from -2 to 2
- mix_gain: float32 [2048], replicated, may hold values from 0.1 to 1.9
- w_query: bfloat16 [2048, 1024], P('ep', 'tp'), may hold values from -0.125 to 0.125
- w_key: bfloat16 [2048, 1024], P('ep', 'tp'), may hold values from -0.125 to 0.125
- w_value: bfloat16 [2048, 2048], P('ep', 'tp'), may hold values from -0.125 to 0.125
- w_input_gate: bfloat16 [2048, 8], replicated, may hold values from -0.125 to 0.125
- w_forget_gate: bfloat16 [2048, 8], replicated, may hold values from -0.125 to 0.125
- forget_bias: float32 [8], replicated, may hold values from -1 to 4
- w_output: bfloat16 [2048, 2048], P('tp', 'ep'), may hold values from -0.125 to 0.125
- moe_gain: float32 [2048], replicated, may hold values from 0.1 to 1.9
- w_group: bfloat16 [2048, 4], replicated, may hold values from -0.25 to 0.25
- expert_ids: int32 [256, 2], P('ep'), may hold values from 0 to 127, all different within a row; in each aligned block of 2 rows (0 to 1, 2 to 3, ...) at most 1 rows name the same one
- expert_weight: float32 [256, 2], P('ep'), may hold values from 0.1 to 1
- w_exp_gate: bfloat16 [128, 2048, 512], P('ep', None, 'tp'), may hold values from -0.125 to 0.125
- w_exp_up: bfloat16 [128, 2048, 512], P('ep', None, 'tp'), may hold values from -0.25 to 0.25
- w_exp_down: bfloat16 [128, 512, 2048], P('ep', 'tp'), may hold values from -1 to 1
- w_dense: bfloat16 [2048, 2048], P('ep', 'tp'), may hold values from -0.125 to 0.125
- w_dense_gate: bfloat16 [2048], replicated, may hold values from -0.125 to 0.125
Outputs:
- mixed: bfloat16 [256, 2048], P('ep', 'tp')
- new_c: float32 [256, 8, 128, 256], P('ep', 'tp')
- new_n: float32 [256, 8, 128], P('ep', 'tp')
- new_m: float32 [256, 8], P('ep', 'tp')
The draws below stay inside these ranges and needn't reach their ends.
Inputs may be any that keep to these rules, and one draw needn't show every extreme that they name: `expert_ids`: each row names 2 different experts. In each aligned block of 2 rows (the rows of one index of ep) no expert is named by more than 1 row, a bound that some block reaches. Every expert is named by some row.
All inputs are finite; a program needn't handle non-finite values.
Results may differ from the reference program's by a relative error of at most 0.025.
Values may be sent and summed in bfloat16 or wider, within the bound.
A program may use at most 64 MiB of HBM per device.

```python
import math
import jax
import jax.numpy as jnp
import numpy as np
from jax import lax

D = 2048
HEADS = 8
DQK = 128
DV = 256
FF = 512
GROUPS = 4
TOPK = 2
SEQ_DEV = 2
SEQS = 256
EXPERTS = 128
CAP = 1
N_TP = 4


def block_levels(own_key, shape, cuts, least, top_value):
    loudness, own = 1.0, jax.random.fold_in(own_key, 6)
    for dim, blocks in cuts:
        heights = jnp.exp(jax.random.uniform(jax.random.fold_in(own, dim), (blocks,), jnp.float32, least / len(cuts), top_value / len(cuts)))
        loudness = loudness * jnp.repeat(heights, shape[dim] // blocks).reshape([-1 if axis == dim else 1 for axis in range(len(shape))])
    return loudness


def assign_block(own_key, own, number, rows, count, top, reach, slope):
    order = jax.random.permutation(own_key, count)
    heavy_load, common = load_shares(count, rows * top, reach, slope, True), load_shares(count, rows * top, reach, slope, False)
    places = jnp.arange(count)

    def named(tallies, offset_by):
        used = int((tallies > 0).sum())
        fixed = max(1, used // 4)
        shifted = fixed + (places - fixed + offset_by * (used - fixed)) % max(1, count - fixed)
        return jnp.zeros((count,), jnp.int32).at[order[jnp.where(places < fixed, places, shifted)]].set(jnp.asarray(tallies, jnp.int32))

    tallies = jnp.where(number % 4 == 0, named(heavy_load, number // 4), named(common, number - number // 4 - 1))
    mixed = jax.random.permutation(jax.random.fold_in(own, 3), count)
    source_of, taker = mixed[0:count // 2 * 2:2], mixed[1:count // 2 * 2:2]
    slack = jnp.minimum(tallies[source_of] - 1, reach - tallies[taker]) // 2
    slack = jnp.where((source_of == order[0]) | (taker == order[0]) | (tallies[taker] == 0), 0, jnp.maximum(slack, 0))
    shifted = jax.random.randint(jax.random.fold_in(own, 4), (count // 2,), 0, 1 << 20) % (slack + 1)
    tallies = tallies.at[source_of].add(-shifted).at[taker].add(shifted)
    members = jnp.searchsorted(jnp.cumsum(tallies), jnp.arange(rows * top), side="right").astype(jnp.int32)
    listing = members.reshape(top, rows).T
    listing = listing[jax.random.permutation(jax.random.fold_in(own, 1), rows)]
    offset_by = jax.random.randint(jax.random.fold_in(own, 2), (rows, 1), 0, top)
    return jnp.take_along_axis(listing, (jnp.arange(top)[None, :] + offset_by) % top, axis=1)


def load_shares(count, total, reach, slope, full):
    portions = [(1 << 20) // math.isqrt(grade ** slope) + 1 for grade in range(1, count + 1)]
    largest = reach if full else min(reach, max(-(-total // count), total * portions[0] // sum(portions)))
    least = 1 if total - largest >= count - 1 else 0
    counts, spare = [largest] + [least] * (count - 1), total - largest - least * (count - 1)
    while spare > 0:
        candidates = [i for i in range(1, count) if counts[i] < largest] or [i for i in range(1, count) if counts[i] < reach]
        whole, left = sum([portions[i] for i in candidates]), spare
        for i in candidates:
            more = min(reach - counts[i], max(1, left * portions[i] // whole), spare)
            counts[i] = counts[i] + more
            spare = spare - more
    return np.array(counts)


def gaussian(own_key, dims, scale, limit, shards=(), kind=jnp.bfloat16):
    result = scale * jax.random.normal(own_key, dims, jnp.float32)
    if shards:
        result = result * block_levels(own_key, dims, shards, -0.22, 0.18)
    return jnp.clip(result, -limit, limit).astype(kind)


def setup_inputs(seed: int = 0) -> dict:
    splits = jax.random.split(jax.random.key(seed), 22)
    tokens = gaussian(splits[0], (SEQS, D), 1.0, 6.0, ((0, 128),))
    state_c = gaussian(splits[1], (SEQS, HEADS, DQK, DV), 0.1, 0.8, ((0, 128), (1, 4)), jnp.float32)
    state_n = gaussian(splits[2], (SEQS, HEADS, DQK), 0.1, 0.8, ((0, 128), (1, 4)), jnp.float32)
    state_m = jnp.clip(jax.random.uniform(splits[3], (SEQS, HEADS), jnp.float32, -2.0, 2.0) * block_levels(splits[3], (SEQS, HEADS), ((0, 128), (1, 4)), -0.4, 0.0), -2.0, 2.0)
    mix_gain = jnp.clip(1.0 + 0.18 * jax.random.normal(splits[4], (D,), jnp.float32), 0.1, 1.9)
    w_query = gaussian(splits[5], (D, HEADS * DQK), D ** -0.5, 0.125, ((0, 128), (1, 4)))
    w_key = gaussian(splits[6], (D, HEADS * DQK), D ** -0.5, 0.125, ((0, 128), (1, 4)))
    w_value = gaussian(splits[7], (D, HEADS * DV), D ** -0.5, 0.125, ((0, 128), (1, 4)))
    w_input_gate = gaussian(splits[8], (D, HEADS), D ** -0.5, 0.125)
    w_forget_gate = gaussian(splits[9], (D, HEADS), D ** -0.5, 0.125)
    forget_bias = jnp.clip(jax.random.uniform(splits[10], (HEADS,), jnp.float32, -1.0, 4.0), -1.0, 4.0)
    w_output = gaussian(splits[11], (HEADS * DV, D), (HEADS * DV) ** -0.5, 0.125, ((0, 4), (1, 128)))
    moe_gain = jnp.clip(1.0 + 0.18 * jax.random.normal(splits[12], (D,), jnp.float32), 0.1, 1.9)
    w_group = gaussian(splits[13], (D, GROUPS), (D // 4) ** -0.5, 0.25)
    expert_ids_keys = jax.random.split(jax.random.fold_in(splits[14], 1), SEQS // SEQ_DEV)
    expert_ids_turns = jax.random.permutation(jax.random.fold_in(splits[14], 3), SEQS // SEQ_DEV)
    expert_ids = jax.vmap(lambda own, number: assign_block(jax.random.fold_in(splits[14], 2), own, number, SEQ_DEV, EXPERTS, TOPK, CAP, 2))(expert_ids_keys, expert_ids_turns).reshape((SEQS, TOPK))
    expert_weight = jnp.clip(jnp.exp(math.log(1.0) - 2.3025851 * jax.random.uniform(splits[15], (SEQS, TOPK), jnp.float32) ** block_levels(splits[15], (SEQS, TOPK), ((0, 128),), -0.2, 0.2)), 0.1, 1.0)
    w_exp_gate = gaussian(splits[16], (EXPERTS, D, FF), D ** -0.5, 0.125, ((0, 128), (2, 4)))
    w_exp_up = gaussian(splits[17], (EXPERTS, D, FF), (D // 4) ** -0.5, 0.25, ((0, 128), (2, 4)))
    w_exp_down = gaussian(splits[18], (EXPERTS, FF, D), (FF // 16) ** -0.5, 1.0, ((0, 128), (1, 4)))
    w_dense = gaussian(splits[19], (D, D), D ** -0.5, 0.125, ((0, 128), (1, 4)))
    w_dense_gate = gaussian(splits[20], (D,), D ** -0.5, 0.125)
    return dict(tokens=tokens, state_c=state_c, state_n=state_n, state_m=state_m, mix_gain=mix_gain, w_query=w_query, w_key=w_key, w_value=w_value, w_input_gate=w_input_gate, w_forget_gate=w_forget_gate, forget_bias=forget_bias, w_output=w_output, moe_gain=moe_gain, w_group=w_group, expert_ids=expert_ids, expert_weight=expert_weight, w_exp_gate=w_exp_gate, w_exp_up=w_exp_up, w_exp_down=w_exp_down, w_dense=w_dense, w_dense_gate=w_dense_gate)


eps = 1e-06

def rms_norm(values, gain):
    widened = values.astype(jnp.float32)
    inverse = lax.rsqrt(lax.optimization_barrier(jnp.mean(widened * widened, axis=-1, keepdims=True)) + eps)
    return (widened * inverse * gain).astype(jnp.bfloat16)

def rounded(values):
    return lax.optimization_barrier(values.astype(jnp.bfloat16)).astype(jnp.float32)

def memory_step(query_rows, key_rows, value_rows, in_gate, forget, state_c, state_n, state_m):
    seq_count, head_count = state_m.shape
    q_heads = query_rows.reshape(seq_count, head_count, -1)
    k_heads = key_rows.reshape(seq_count, head_count, -1) * q_heads.shape[-1] ** (-0.5)
    v_heads = value_rows.reshape(seq_count, head_count, -1)
    new_m = jnp.maximum(forget + state_m, in_gate)
    decay = jnp.exp(forget + state_m - new_m)
    inflow = jnp.exp(in_gate - new_m)
    new_c = decay[..., None, None] * state_c + (inflow[..., None] * k_heads)[..., :, None] * v_heads[..., None, :]
    new_n = decay[..., None] * state_n + inflow[..., None] * k_heads
    numer = jnp.einsum('shd,shde->she', q_heads, new_c, precision=lax.Precision.HIGHEST)
    denom = jnp.maximum(jnp.abs(lax.optimization_barrier(jnp.sum(q_heads * new_n, axis=-1))), 1.0)
    heads = (numer / denom[..., None]).astype(jnp.bfloat16).reshape(seq_count, -1)
    return (heads, new_c, new_n, new_m)

def reference(tokens, state_c, state_n, state_m, mix_gain, w_query, w_key, w_value, w_input_gate, w_forget_gate, forget_bias, w_output, moe_gain, w_group, expert_ids, expert_weight, w_exp_gate, w_exp_up, w_exp_down, w_dense, w_dense_gate):
    seq_count = tokens.shape[0]
    normed = rms_norm(tokens, mix_gain)
    query_rows = rounded(jnp.dot(normed, w_query, preferred_element_type=jnp.float32))
    key_rows = rounded(jnp.dot(normed, w_key, preferred_element_type=jnp.float32))
    value_rows = rounded(jnp.dot(normed, w_value, preferred_element_type=jnp.float32))
    in_gate = jnp.dot(normed, w_input_gate, preferred_element_type=jnp.float32)
    forget = jax.nn.log_sigmoid(jnp.dot(normed, w_forget_gate, preferred_element_type=jnp.float32) + forget_bias)
    heads, new_c, new_n, new_m = memory_step(query_rows, key_rows, value_rows, in_gate, forget, state_c, state_n, state_m)
    head_blocks = heads.reshape(seq_count, N_TP, -1).astype(jnp.float32)
    out_blocks = w_output.reshape(N_TP, -1, D).astype(jnp.float32)
    partials = rounded(jnp.einsum('stf,tfd->tsd', head_blocks, out_blocks))
    residual = (tokens.astype(jnp.float32) + lax.optimization_barrier(jnp.sum(partials, axis=0))).astype(jnp.bfloat16)
    normed2 = rms_norm(residual, moe_gain)
    group_prob = jax.nn.softmax(jnp.dot(normed2, w_group, preferred_element_type=jnp.float32), axis=-1)
    per_group = EXPERTS // GROUPS
    member = (expert_ids // per_group)[..., None] == jnp.arange(GROUPS, dtype=jnp.int32)[None, None, :]
    picked = lax.optimization_barrier(jnp.sum(jnp.where(member, group_prob[:, None, :], 0.0), axis=-1))
    route = picked * expert_weight / lax.optimization_barrier(jnp.sum(expert_weight, axis=1, keepdims=True))
    flat_ids = expert_ids.reshape(-1).astype(jnp.int32)
    repeated = jnp.repeat(normed2, TOPK, axis=0)

    def run_one(item):
        ident, token_row = item
        gate_matrix = lax.dynamic_index_in_dim(w_exp_gate, ident, 0, keepdims=False)
        up_matrix = lax.dynamic_index_in_dim(w_exp_up, ident, 0, keepdims=False)
        down_matrix = lax.dynamic_index_in_dim(w_exp_down, ident, 0, keepdims=False)
        gate_act = jnp.dot(token_row[None, :], gate_matrix, preferred_element_type=jnp.float32)
        up_act = jnp.dot(token_row[None, :], up_matrix, preferred_element_type=jnp.float32)
        hidden = (jax.nn.silu(gate_act) * up_act).astype(jnp.bfloat16)
        hidden_blocks = hidden.reshape(N_TP, -1).astype(jnp.float32)
        down_blocks = down_matrix.reshape(N_TP, -1, D).astype(jnp.float32)
        parts = rounded(jnp.einsum('tf,tfd->td', hidden_blocks, down_blocks))
        return lax.optimization_barrier(jnp.sum(parts, axis=0)).astype(jnp.bfloat16)
    expert_out = lax.map(run_one, (flat_ids, repeated))
    moe = lax.optimization_barrier(jnp.sum(route[..., None] * expert_out.astype(jnp.float32).reshape(seq_count, TOPK, D), axis=1))
    dense_gate = jax.nn.sigmoid(jnp.dot(normed2, w_dense_gate, preferred_element_type=jnp.float32))
    dense = dense_gate[:, None] * jnp.dot(normed2, w_dense, preferred_element_type=jnp.float32)
    mixed = (residual.astype(jnp.float32) + moe + dense).astype(jnp.bfloat16)
    return (mixed, new_c, new_n, new_m)
```

```python
import jax
import jax.numpy as jnp
from jax import lax
from jax.experimental import pallas as pl
from jax.experimental.pallas import tpu as pltpu
from jax.sharding import PartitionSpec as P

NY = 8
NC = 2
eps = 1e-06
BF = jnp.bfloat16
F32 = jnp.float32
MESH = pl.DeviceIdType.MESH
NN = (((1,), (0,)), ((), ()))
NT = (((1,), (1,)), ((), ()))
TN = (((0,), (0,)), ((), ()))


def mm(a, b, dims=NN, precision=None):
    return lax.dot_general(a, b, dims, precision=precision, preferred_element_type=F32)


def iota(shape, dim):
    return lax.broadcasted_iota(jnp.int32, shape, dim)


def ones_where(mask):
    return jnp.where(mask, 1.0, 0.0).astype(BF)


def each(count, body):
    def step(d, carry):
        body(d)
        return carry

    lax.fori_loop(1, count, step, 0)


def wait_for(ref, sem):
    pltpu.make_async_copy(ref, ref, sem).wait()


def layer_kernel(
    n_ep,
    n_tp,
    tokens,
    state_c,
    state_n,
    state_m,
    mix_gain,
    w_query,
    w_key,
    w_value,
    w_in,
    w_forget,
    forget_bias,
    w_out,
    moe_gain,
    w_group,
    expert_ids,
    expert_weight,
    w_gate,
    w_up,
    w_down,
    w_dense,
    w_dense_gate,
    mixed,
    new_c,
    new_n,
    new_m,
    nrm,
    tn,
    tr,
    meta_own,
    meta,
    wqkv,
    wot,
    wd,
    pb,
    rb,
    c_in,
    c_out,
    hb,
    hg,
    op,
    og,
    res,
    ag,
    n2,
    n2z,
    wg,
    wu,
    wdn,
    dp,
    xg,
    eo,
    zg,
    ys,
    yg,
    loads,
    sent,
    got,
    got_z,
    count,
):
    nz = n_ep // (NY * NC)
    rows = w_query.shape[0]
    width = tokens.shape[1]
    block = NY * NC * rows
    nzc, nyc = nz * NC, NY * NC
    half = nz * NC
    seqs = 2 * n_ep
    share = width // n_tp
    qk = w_query.shape[1]
    lanes = wd.shape[1]
    group_count = w_group.shape[0]

    ep = lax.axis_index("ep")
    x = lax.axis_index("tp")
    z = ep // nyc
    y = (ep // NC) % NY
    c = ep % NC
    zc = z * NC + c
    yc = y * NC + c

    def device(z_, y_, c_, x_):
        return {"ep": (z_ * NY + y_) * NC + c_, "tp": x_}

    def send(src, dst, s, r, to):
        pltpu.make_async_remote_copy(
            src_ref=src, dst_ref=dst, send_sem=s, recv_sem=r, device_id=to, device_id_type=MESH
        ).start()

    def y_peer(d):
        return device(z, (y + d) % NY, c, x)

    def zc_peer(d):
        other = (zc + d) % nzc
        return other // NC, other, device(other // NC, y, other % NC, x)

    def xc_peer(d):
        other = (x * NC + c + d) % (n_tp * NC)
        return device(z, y, other % NC, other // NC)

    load_c = pltpu.make_async_copy(state_c, c_in, loads.at[0])
    load_g = pltpu.make_async_copy(w_gate.at[0], wg, loads.at[1])
    load_u = pltpu.make_async_copy(w_up.at[0], wu, loads.at[2])
    load_d = pltpu.make_async_copy(w_down.at[0], wdn, loads.at[3])
    for copy in (load_c, load_g, load_u, load_d):
        copy.start()

    wqkv[...] = jnp.zeros_like(wqkv)
    wot[...] = jnp.zeros_like(wot)
    wd[...] = jnp.zeros_like(wd)

    barrier = pltpu.get_barrier_semaphore()

    def greet(to):
        pl.semaphore_signal(barrier, inc=1, device_id=to, device_id_type=MESH)

    each(NY, lambda d: greet(y_peer(d)))
    each(nzc, lambda d: greet(zc_peer(d)[2]))
    each(n_tp * NC, lambda d: greet(xc_peer(d)))

    wide = tokens[...].astype(F32)
    inverse = lax.rsqrt(jnp.mean(wide * wide, axis=-1, keepdims=True) + eps)
    nrm[...] = jnp.zeros_like(nrm)
    nrm[0:2, :] = (wide * inverse * mix_gain[...]).astype(BF)
    lane = iota((2, 128), 1)
    idf = expert_ids[...].astype(F32)
    ewt = expert_weight[...]
    ew_hi = ewt.astype(BF).astype(F32)
    ew_lo = ewt - ew_hi
    packed = jnp.zeros((2, 128), F32)
    for k, part in enumerate((idf, ew_hi, ew_lo)):
        for j in range(2):
            packed = jnp.where(lane == 2 * k + j, part[:, j : j + 1], packed)
    meta_own[...] = jnp.zeros_like(meta_own)
    meta_own[0:2, :] = packed.astype(BF)

    own = pl.ds(pl.multiple_of(yc * rows, rows), rows)
    wqkv[own, 0:qk] = w_query[...]
    wqkv[own, qk : 2 * qk] = w_key[...]
    wqkv[own, 2 * qk :] = w_value[...]
    wot[own, :] = w_out[...]
    start = yc * rows
    dense_block = start // lanes
    dense_rows = pl.ds(pl.multiple_of(start % lanes, rows), rows)
    wd[z, dense_rows, :] = w_dense[...]

    pl.semaphore_wait(barrier, (NY - 1) + (nzc - 1) + (n_tp * NC - 1))

    def send_projection(d):
        to = y_peer(d)
        send(w_query, wqkv.at[own, pl.ds(0, qk)], sent.at[0], got.at[0], to)
        send(w_key, wqkv.at[own, pl.ds(qk, qk)], sent.at[0], got.at[0], to)
        send(w_value, wqkv.at[own, pl.ds(2 * qk, 2 * qk)], sent.at[0], got.at[0], to)

    def pair(index):
        return pl.ds(pl.multiple_of(2 * index, 2), 2)

    def cols(index):
        return pl.ds(pl.multiple_of(index * block, block), block)

    def send_rows(d):
        z_, _, to = zc_peer(d)
        send(nrm.at[0:2, cols(z_)], tn.at[pair(zc), :], sent.at[1], got.at[1], to)

    def send_raw(d):
        z_, _, to = zc_peer(d)
        send(tokens.at[:, cols(z_)], tr.at[pair(zc), :], sent.at[2], got.at[2], to)
        send(meta_own.at[0:2, :], meta.at[y, pair(zc), :], sent.at[3], got.at[3], to)

    each(nzc, send_rows)
    each(NY, send_projection)
    each(NY, lambda d: send(w_out, wot.at[own, :], sent.at[4], got.at[4], y_peer(d)))
    each(nzc, send_raw)
    each(
        nz,
        lambda d: send(
            w_dense,
            wd.at[z, dense_rows, :],
            sent.at[5],
            got.at[5],
            device((z + d) % nz, y, c, x),
        ),
    )
    keep_n = pltpu.make_async_copy(nrm.at[0:2, cols(z)], tn.at[pair(zc), :], loads.at[4])
    keep_r = pltpu.make_async_copy(tokens.at[:, cols(z)], tr.at[pair(zc), :], loads.at[5])
    keep_m = pltpu.make_async_copy(meta_own.at[0:2, :], meta.at[y, pair(zc), :], loads.at[6])
    for copy in (keep_n, keep_r, keep_m):
        copy.start()

    head_count = state_m.shape[1]
    gate_all = mm(nrm[...], w_in[...], NT)[0:2]
    raw = mm(nrm[...], w_forget[...], NT)[0:2] + forget_bias[...]
    forget_all = jnp.minimum(raw, 0.0) - jnp.log1p(jnp.exp(-jnp.abs(raw)))
    head_lane = iota(gate_all.shape, 1)

    def of_head(values, h):
        mine = head_lane == x * head_count + h
        return jnp.sum(jnp.where(mine, values, 0.0), axis=1, keepdims=True)

    decays, inflows, ms = [], [], []
    for h in range(head_count):
        gate_h, forget_h = of_head(gate_all, h), of_head(forget_all, h)
        kept = forget_h + state_m[:, h : h + 1]
        m_h = jnp.maximum(kept, gate_h)
        decays.append(jnp.exp(kept - m_h))
        inflows.append(jnp.exp(gate_h - m_h))
        ms.append(m_h)
    m_lane = iota(state_m.shape, 1)
    new_m_value = jnp.zeros(state_m.shape, F32)
    for h in range(head_count):
        new_m_value = jnp.where(m_lane == h, ms[h], new_m_value)
    new_m[...] = new_m_value

    keep_m.wait()
    wait_for(count.at[0 : nzc - 1, :, 0:128], got.at[3])
    each(NY, lambda d: send(meta.at[y], meta.at[y], sent.at[6], got.at[6], y_peer(d)))

    keep_n.wait()
    wait_for(count.at[0 : nzc - 1, :, 0:block], got.at[1])
    wait_for(wqkv.at[0 : (NY - 1) * rows, :], got.at[0])
    pb[...] = mm(tn[...], wqkv[...]).astype(BF)
    keep_p = pltpu.make_async_copy(pb.at[pair(zc), :], rb.at[pair(zc), :], loads.at[4])
    keep_p.start()

    def send_partial(d):
        _, other, to = zc_peer(d)
        send(pb.at[pair(other), :], rb.at[pair(zc), :], sent.at[7], got.at[7], to)

    each(nzc, send_partial)
    load_c.wait()
    keep_p.wait()
    wait_for(count.at[0 : nzc - 1, :, 0:4 * qk], got.at[7])

    def pair_sum(count):
        r, col = iota((16, 2 * count), 0), iota((16, 2 * count), 1)
        return ones_where((col & 1) == r)

    rows_sum = mm(pair_sum(nzc), rb[...]).astype(BF)

    row = iota((16, 1), 0)
    dqk, dv = state_c.shape[2], state_c.shape[3]
    for h in range(head_count):
        q = rows_sum[:, h * dqk : (h + 1) * dqk]
        k = rows_sum[:, qk + h * dqk : qk + (h + 1) * dqk]
        v = rows_sum[:, 2 * qk + h * dv : 2 * qk + (h + 1) * dv]
        qf, kf = q.astype(F32), k.astype(F32)
        heads = jnp.zeros((16, dv), F32)
        for t in range(2):
            decay = decays[h][t : t + 1, :]
            inflow = inflows[h][t : t + 1, :] * dqk ** (-0.5)
            outer = mm(jnp.where(row == t, kf, 0.0).astype(BF), v, TN)
            c_new = decay * c_in[t, h] + inflow * outer
            c_out[t, h] = c_new
            n_new = decay * state_n[t, h : h + 1, :] + inflow * kf[t : t + 1, :]
            new_n[t, h : h + 1, :] = n_new
            numer = mm(qf, c_new, precision=lax.Precision.HIGHEST)
            denom = jnp.sum(qf[t : t + 1, :] * n_new, axis=-1, keepdims=True)
            denom = jnp.maximum(jnp.abs(denom), 1.0)
            heads = jnp.where(row == t, numer / denom, heads)
        hb[:, h * dv : (h + 1) * dv] = heads.astype(BF)
    store_c = pltpu.make_async_copy(c_out, new_c, loads.at[0])
    store_c.start()

    keep_h = pltpu.make_async_copy(hb.at[0:2, :], hg.at[pair(zc), :], loads.at[4])
    keep_h.start()
    each(
        nzc,
        lambda d: send(
            hb.at[0:2, :], hg.at[pair(zc), :], sent.at[8], got.at[8], zc_peer(d)[2]
        ),
    )
    wait_for(wot.at[0 : (NY - 1) * rows, :], got.at[4])
    keep_r.wait()
    wait_for(count.at[0 : nzc - 1, :, 0:block], got.at[2])
    keep_h.wait()
    wait_for(count.at[0 : nzc - 1, :, 0:2 * qk], got.at[8])
    part = mm(hg[...], wot[...], NT).astype(BF)
    op[...] = part
    xc = x * NC + c
    og[xc] = part
    each(n_tp * NC, lambda d: send(op, og.at[xc], sent.at[9], got.at[9], xc_peer(d)))
    wait_for(og.at[0 : n_tp * NC - 1], got.at[9])
    parts = jnp.zeros((2 * nzc, block), F32)
    for k in range(n_tp * NC):
        parts = parts + og[k].astype(F32)
    res[...] = (tr[...].astype(F32) + parts).astype(BF)

    sa = z + c * (y - z)
    sb = y + c * (z - y)

    def at(a, b):
        return device(a + c * (b - a), b + c * (a - b), c, x)

    ag[c, sa, sb] = res[pl.ds(pl.multiple_of(c * half, half), half), :]
    mine = ag.at[c, sa, sb]
    each(NY, lambda d: send(mine, mine, sent.at[10], got.at[10], at(sa, (sb + d) % NY)))
    wait_for(ag.at[0, 0, 0 : NY - 1], got.at[10])
    line = ag.at[c, sa]
    partner = device(z, y, 1 - c, x)
    each(nz, lambda d: send(line, line, sent.at[11], got_z.at[d], at((sa + d) % nz, sb)))
    send(line, line, sent.at[12], got.at[11], partner)

    def pass_on(d):
        arrived = ag.at[c, (sa + nz - d) % nz]
        wait_for(arrived, got_z.at[d])
        send(arrived, arrived, sent.at[12], got.at[11], partner)

    each(nz, pass_on)
    wait_for(meta.at[0 : NY - 1], got.at[6])
    for copy in (load_g, load_u, load_d):
        copy.wait()
    wait_for(ag.at[0], got.at[11])

    side = seqs // 2

    def rows_of(h, b):
        values = ag[0, b] if h == 0 else ag[1, :, b]
        return values.reshape(side, block)

    for h in range(2):
        squares = jnp.zeros((side, block), F32)
        for b in range(nz):
            piece = rows_of(h, b).astype(F32)
            squares = squares + piece * piece
        mean = jnp.sum(squares, axis=-1, keepdims=True) * (1.0 / width)
        inverse = lax.rsqrt(mean + eps)
        for b in range(nz):
            piece = rows_of(h, b).astype(F32)
            gain = moe_gain[:, b * block : (b + 1) * block]
            n2[h * side : (h + 1) * side, b * block : (b + 1) * block] = (
                piece * inverse * gain
            ).astype(BF)

    gate_act = mm(n2[...], wg[...])
    up_act = mm(n2[...], wu[...])
    hidden = gate_act * jax.nn.sigmoid(gate_act) * up_act
    meta_rows = jnp.concatenate(
        [meta[:, h * half : (h + 1) * half, :].reshape(side, 128) for h in range(2)], axis=0
    )
    mf = meta_rows.astype(F32)
    expert = ep.astype(F32)
    assigned = (mf[:, 0:1] == expert) | (mf[:, 1:2] == expert)
    hidden = jnp.where(assigned, hidden, 0.0).astype(BF)

    def token_of(shape):
        r = iota(shape, 1)
        h, y_, rest = r // side, (r // half) % NY, r % half
        z_ = h * (nz // 2) + rest // (2 * NC)
        return ((z_ * NY + y_) * NC) * 2 + rest % (2 * NC)

    slot_rows = iota((n_ep, seqs), 0)
    placing = ones_where(token_of((n_ep, seqs)) // 2 == slot_rows)
    slots = mm(placing, hidden).astype(BF)

    def down(x_):
        return mm(slots, wdn[:, pl.ds(pl.multiple_of(x_ * share, share), share)]).astype(BF)

    for d in range(1, n_tp):
        x_ = (x + d) % n_tp
        dp[d] = down(x_)
        send(dp.at[d], xg.at[x], sent.at[13], got.at[12], device(z, y, c, x_))
    xg[x] = down(x)

    local = ones_where(token_of((2 * nyc, seqs)) == z * 2 * nyc + iota((2 * nyc, seqs), 0))
    picks = mm(local, meta_rows)
    zrows = mm(local, n2[...]).astype(BF)
    n2z[...] = zrows
    wait_for(wd.at[0 : nz - 1, 0:rows, :], got.at[5])
    dense = jnp.zeros((2 * nyc, share), F32)
    for b in range(nz):
        at_lane = pl.multiple_of(b * block + dense_block * lanes, lanes)
        dense = dense + mm(n2z[:, pl.ds(at_lane, lanes)], wd[b])
    dense_gate = jnp.sum(
        zrows.astype(F32) * w_dense_gate[...].astype(F32), axis=-1, keepdims=True
    )
    dense = jax.nn.sigmoid(dense_gate) * dense
    logits = mm(zrows, w_group[...], NT)
    shifted = jnp.exp(logits - jnp.max(logits, axis=-1, keepdims=True))
    prob = shifted / jnp.sum(shifted, axis=-1, keepdims=True)
    per_group = n_ep // group_count
    first = (iota(prob.shape, 1) * per_group).astype(F32)
    weights = [picks[:, 2 + j : 3 + j] + picks[:, 4 + j : 5 + j] for j in range(2)]
    total = weights[0] + weights[1]
    at_slot = iota((2 * nyc, n_ep), 1)
    source = ((at_slot // nyc) * nyc + yc).astype(F32)
    same = at_slot % nyc == iota((2 * nyc, n_ep), 0) // 2
    mixing = jnp.zeros((2 * nyc, n_ep), F32)
    for j in range(2):
        ident = picks[:, j : j + 1]
        member = (ident >= first) & (ident < first + per_group)
        picked = jnp.sum(jnp.where(member, prob, 0.0), axis=-1, keepdims=True)
        route = picked * weights[j] / total
        mixing = mixing + jnp.where(same & (ident == source), route, 0.0)
    mix_hi = mixing.astype(BF)
    mix_lo = (mixing - mix_hi.astype(F32)).astype(BF)
    owned = ones_where(
        (token_of((16, seqs)) == 2 * ep + iota((16, seqs), 0)) & (iota((16, seqs), 0) < 2)
    )
    per_share = nz // n_tp
    residual = []
    for k in range(per_share):
        b = x * per_share + k
        residual.append(
            mm(owned[:, 0:side], ag[0, b].reshape(side, block))
            + mm(owned[:, side:], ag[1, :, b].reshape(side, block))
        )

    wait_for(xg.at[0 : n_tp - 1], got.at[12])
    total_out = xg[0].astype(F32)
    for k in range(1, n_tp):
        total_out = total_out + xg[k].astype(F32)
    eo[...] = total_out.astype(BF)

    def slots_of(z_):
        return eo.at[pl.ds(pl.multiple_of(z_ * nyc, nyc), nyc), :]

    each(
        nz,
        lambda d: send(
            slots_of((z + d) % nz), zg.at[z], sent.at[14], got.at[13], device((z + d) % nz, y, c, x)
        ),
    )
    zg[z] = eo[pl.ds(pl.multiple_of(z * nyc, nyc), nyc), :]
    wait_for(zg.at[0 : nz - 1], got.at[13])
    arrived = zg[...].reshape(n_ep, share)
    ys[...] = (mm(mix_hi, arrived) + mm(mix_lo, arrived) + dense).astype(BF)
    keep_y = pltpu.make_async_copy(ys.at[pair(yc), :], yg.at[pair(yc), :], loads.at[4])
    keep_y.start()

    def send_sums(d):
        other = (yc + d) % nyc
        to = device(z, other // NC, other % NC, x)
        send(ys.at[pair(other), :], yg.at[pair(yc), :], sent.at[15], got.at[14], to)

    each(nyc, send_sums)
    keep_y.wait()
    wait_for(count.at[0 : nyc - 1, :, 0:share], got.at[14])
    summed = mm(pair_sum(nyc), yg[...])
    for k in range(per_share):
        at_cols = slice(k * block, (k + 1) * block)
        mixed[:, at_cols] = (residual[k] + summed[:, at_cols])[0:2].astype(BF)

    store_c.wait()
    wait_for(wqkv.at[0 : (NY - 1) * rows, :], sent.at[0])
    wait_for(count.at[0 : nzc - 1, :, 0:block], sent.at[1])
    wait_for(count.at[0 : nzc - 1, :, 0:block], sent.at[2])
    wait_for(count.at[0 : nzc - 1, :, 0:128], sent.at[3])
    wait_for(wot.at[0 : (NY - 1) * rows, :], sent.at[4])
    wait_for(wd.at[0 : nz - 1, 0:rows, :], sent.at[5])
    wait_for(meta.at[0 : NY - 1], sent.at[6])
    wait_for(count.at[0 : nzc - 1, :, 0:4 * qk], sent.at[7])
    wait_for(count.at[0 : nzc - 1, :, 0:2 * qk], sent.at[8])
    wait_for(og.at[0 : n_tp * NC - 1], sent.at[9])
    wait_for(ag.at[0, 0, 0 : NY - 1], sent.at[10])
    wait_for(ag.at[0, 0 : nz - 1], sent.at[11])
    wait_for(ag.at[0], sent.at[12])
    wait_for(xg.at[0 : n_tp - 1], sent.at[13])
    wait_for(zg.at[0 : nz - 1], sent.at[14])
    wait_for(count.at[0 : nyc - 1, :, 0:share], sent.at[15])


def per_device(
    tokens,
    state_c,
    state_n,
    state_m,
    mix_gain,
    w_query,
    w_key,
    w_value,
    w_input_gate,
    w_forget_gate,
    forget_bias,
    w_output,
    moe_gain,
    w_group,
    expert_ids,
    expert_weight,
    w_exp_gate,
    w_exp_up,
    w_exp_down,
    w_dense,
    w_dense_gate,
):
    n_ep, n_tp = lax.axis_size("ep"), lax.axis_size("tp")
    nz = n_ep // (NY * NC)
    width = tokens.shape[1]
    rows = w_query.shape[0]
    block = NY * NC * rows
    lanes = min(128, block)
    share = width // n_tp
    nzc, nyc = nz * NC, NY * NC
    hidden = w_exp_gate.shape[2]
    qkv = 2 * w_query.shape[1] + w_value.shape[1]
    vm = pl.BlockSpec(memory_space=pltpu.VMEM)
    anywhere = pl.BlockSpec(memory_space=pl.ANY)
    V = pltpu.VMEM

    def kernel(*refs):
        layer_kernel(n_ep, n_tp, *refs)

    in_specs = [vm] * 21
    for k in (1, 16, 17, 18):
        in_specs[k] = anywhere
    out_shape = (
        jax.ShapeDtypeStruct((2, share), BF),
        jax.ShapeDtypeStruct(state_c.shape, F32),
        jax.ShapeDtypeStruct(state_n.shape, F32),
        jax.ShapeDtypeStruct(state_m.shape, F32),
    )
    scratch = [
        V((16, width), BF),
        V((2 * nzc, block), BF),
        V((2 * nzc, block), BF),
        V((16, 128), BF),
        V((NY, 2 * nzc, 128), BF),
        V((block, qkv), BF),
        V((block, w_output.shape[0]), BF),
        V((nz, lanes, share), BF),
        V((2 * nzc, qkv), BF),
        V((2 * nzc, qkv), BF),
        V(state_c.shape, F32),
        V(state_c.shape, F32),
        V((16, w_output.shape[0]), BF),
        V((2 * nzc, w_output.shape[0]), BF),
        V((2 * nzc, block), BF),
        V((n_tp * NC, 2 * nzc, block), BF),
        V((2 * nzc, block), BF),
        V((2, nz, NY, nzc, block), BF),
        V((2 * n_ep, width), BF),
        V((2 * nyc, width), BF),
        V((width, hidden), BF),
        V((width, hidden), BF),
        V((hidden, width), BF),
        V((n_tp, n_ep, share), BF),
        V((n_tp, n_ep, share), BF),
        V((n_ep, share), BF),
        V((nz, nyc, share), BF),
        V((2 * nyc, share), BF),
        V((2 * nyc, share), BF),
        pltpu.SemaphoreType.DMA((8,)),
        pltpu.SemaphoreType.DMA((16,)),
        pltpu.SemaphoreType.DMA((16,)),
        pltpu.SemaphoreType.DMA((nz,)),
        V((max(nzc, nyc), 2, qkv), BF),
    ]
    return pl.pallas_call(
        kernel,
        name="layer",
        out_shape=out_shape,
        in_specs=in_specs,
        out_specs=(vm, anywhere, vm, vm),
        scratch_shapes=scratch,
        compiler_params=pltpu.CompilerParams(
            collective_id=0, has_side_effects=True, vmem_limit_bytes=40 * 1024 * 1024
        ),
    )(
        tokens,
        state_c,
        state_n,
        state_m,
        mix_gain.reshape(1, -1),
        w_query,
        w_key,
        w_value,
        w_input_gate.T,
        w_forget_gate.T,
        forget_bias.reshape(1, -1),
        w_output.T,
        moe_gain.reshape(1, -1),
        w_group.T,
        expert_ids,
        expert_weight,
        w_exp_gate,
        w_exp_up,
        w_exp_down,
        w_dense,
        w_dense_gate.reshape(1, -1),
    )


def solution(mesh):
    placed = (
        P("ep", None),
        P("ep", "tp", None, None),
        P("ep", "tp", None),
        P("ep", "tp"),
        P(),
        P("ep", "tp"),
        P("ep", "tp"),
        P("ep", "tp"),
        P(),
        P(),
        P(),
        P("tp", "ep"),
        P(),
        P(),
        P("ep", None),
        P("ep", None),
        P("ep", None, "tp"),
        P("ep", None, "tp"),
        P("ep", "tp", None),
        P("ep", "tp"),
        P(),
    )
    return jax.shard_map(
        per_device,
        mesh=mesh,
        in_specs=placed,
        out_specs=(P("ep", "tp"), P("ep", "tp", None, None), P("ep", "tp", None), P("ep", "tp")),
        check_vma=False,
    )
```

```python
import jax
import jax.numpy as jnp
from jax import lax
from jax.experimental import pallas as pl
from jax.experimental.pallas import tpu as pltpu
from jax.sharding import PartitionSpec as P

NY = 8
NC = 2
eps = 1e-06
BF = jnp.bfloat16
F32 = jnp.float32
MESH = pl.DeviceIdType.MESH
NN = (((1,), (0,)), ((), ()))
NT = (((1,), (1,)), ((), ()))
TN = (((0,), (0,)), ((), ()))


def mm(a, b, dims=NN, precision=None):
    return lax.dot_general(a, b, dims, precision=precision, preferred_element_type=F32)


def iota(shape, dim):
    return lax.broadcasted_iota(jnp.int32, shape, dim)


def ones_where(mask):
    return jnp.where(mask, 1.0, 0.0).astype(BF)


def each(count, body):
    def step(d, carry):
        body(d)
        return carry

    lax.fori_loop(1, count, step, 0)


def wait_for(ref, sem):
    pltpu.make_async_copy(ref, ref, sem).wait()


def layer_kernel(
    n_ep,
    n_tp,
    tokens_h,
    state_c_h,
    state_n_h,
    state_m_h,
    mix_gain_h,
    w_query_h,
    w_key_h,
    w_value_h,
    w_in_h,
    w_forget_h,
    forget_bias_h,
    w_out_h,
    moe_gain_h,
    w_group_h,
    expert_ids_h,
    expert_weight_h,
    w_gate_h,
    w_up_h,
    w_down_h,
    w_dense_h,
    w_dense_gate_h,
    mixed,
    new_c,
    new_n,
    new_m,
    nrm,
    nrmh,
    tn,
    tny,
    tr,
    meta_own,
    meta,
    wqk,
    wv,
    wot,
    wd,
    pb,
    rb,
    pbv,
    rbv,
    c_in,
    c_out,
    hb,
    hg,
    op,
    og,
    ag,
    n2,
    hidden,
    meta_rows,
    n2z,
    wg,
    wu,
    wdn,
    dp,
    xg,
    eo,
    zg,
    ys,
    yg,
    loads,
    sent,
    got,
    got_z,
    got_far,
    got_y,
    got_x,
    count,
    tokens,
    state_n,
    state_m,
    mix_gain,
    w_in,
    w_forget,
    forget_bias,
    moe_gain,
    w_group,
    expert_ids,
    expert_weight,
    w_dense_gate,
):
    nz = n_ep // (NY * NC)
    rows = w_query_h.shape[0]
    width = tokens.shape[1]
    block = NY * NC * rows
    nzc, nyc = nz * NC, NY * NC
    half = nz * NC
    seqs = 2 * n_ep
    share = width // n_tp
    qk = w_query_h.shape[1]
    lanes = wd.shape[1]
    group_count = w_group.shape[0]

    ep = lax.axis_index("ep")
    x = lax.axis_index("tp")
    z = ep // nyc
    y = (ep // NC) % NY
    c = ep % NC
    zc = z * NC + c
    yc = y * NC + c

    def device(z_, y_, c_, x_):
        return {"ep": (z_ * NY + y_) * NC + c_, "tp": x_}

    def send(src, dst, s, r, to):
        pltpu.make_async_remote_copy(
            src_ref=src, dst_ref=dst, send_sem=s, recv_sem=r, device_id=to, device_id_type=MESH
        ).start()

    def y_peer(d):
        return device(z, (y + d) % NY, c, x)

    def zc_peer(d):
        other = (zc + d) % nzc
        return other // NC, other, device(other // NC, y, other % NC, x)

    def yc_peer(d):
        other = (yc + d) % nyc
        return other, device(z, other // NC, other % NC, x)

    def xc_peer(d):
        other = (x * NC + c + d) % (n_tp * NC)
        return device(z, y, other % NC, other // NC)

    started = {}

    def load(name, src, dst):
        started[name] = pltpu.make_async_copy(src, dst, loads.at[8 + len(started)])
        started[name].start()

    load("tokens", tokens_h, tokens)
    load("mix_gain", mix_gain_h, mix_gain)
    load("expert_ids", expert_ids_h, expert_ids)
    load("expert_weight", expert_weight_h, expert_weight)

    wqk[...] = jnp.zeros_like(wqk)
    wv[...] = jnp.zeros_like(wv)
    wot[...] = jnp.zeros_like(wot)
    wd[...] = jnp.zeros_like(wd)
    own = pl.ds(pl.multiple_of(yc * rows, rows), rows)
    start = yc * rows
    dense_block = start // lanes
    dense_rows = pl.ds(pl.multiple_of(start % lanes, rows), rows)
    load("w_query", w_query_h, wqk.at[own, 0:qk])
    load("w_key", w_key_h, wqk.at[own, qk : 2 * qk])
    load("w_value", w_value_h, wv.at[z, dense_rows, :])
    load("w_out", w_out_h, wot.at[own, :])
    load("w_dense", w_dense_h, wd.at[z, dense_rows, :])
    load("w_in", w_in_h, w_in)
    load("w_forget", w_forget_h, w_forget)
    load("forget_bias", forget_bias_h, forget_bias)
    load("state_m", state_m_h, state_m)
    load("state_n", state_n_h, state_n)
    load("state_c", state_c_h, c_in)
    load("moe_gain", moe_gain_h, moe_gain)
    load("w_group", w_group_h, w_group)
    load("w_dense_gate", w_dense_gate_h, w_dense_gate)
    load("w_gate", w_gate_h.at[0], wg)
    load("w_up", w_up_h.at[0], wu)
    load("w_down", w_down_h.at[0], wdn)

    def loaded(*names):
        for name in names:
            started[name].wait()

    barrier = pltpu.get_barrier_semaphore()

    def greet(to):
        pl.semaphore_signal(barrier, inc=1, device_id=to, device_id_type=MESH)

    each(nyc, lambda d: greet(yc_peer(d)[1]))
    each(nzc, lambda d: greet(zc_peer(d)[2]))
    each(n_tp * NC, lambda d: greet(xc_peer(d)))

    loaded("tokens", "mix_gain", "expert_ids", "expert_weight")
    wide = tokens[...].astype(F32)
    inverse = lax.rsqrt(jnp.mean(wide * wide, axis=-1, keepdims=True) + eps)
    nrm[...] = jnp.zeros_like(nrm)
    normed = (wide * inverse * mix_gain[...]).astype(BF)
    nrm[0:2, :] = normed
    for k in range(block // lanes):
        for b in range(nz):
            first = b * block + k * lanes
            nrmh[k, 0:2, b * lanes : (b + 1) * lanes] = normed[:, first : first + lanes]
    lane = iota((2, 128), 1)
    idf = expert_ids[...].astype(F32)
    ewt = expert_weight[...]
    ew_hi = ewt.astype(BF).astype(F32)
    ew_lo = ewt - ew_hi
    packed = jnp.zeros((2, 128), F32)
    for k, part in enumerate((idf, ew_hi, ew_lo)):
        for j in range(2):
            packed = jnp.where(lane == 2 * k + j, part[:, j : j + 1], packed)
    meta_own[...] = jnp.zeros_like(meta_own)
    meta_own[0:2, :] = packed.astype(BF)

    loaded("w_query", "w_key", "w_value", "w_out", "w_dense")
    pl.semaphore_wait(barrier, (nyc - 1) + (nzc - 1) + (n_tp * NC - 1))

    def pair(index):
        return pl.ds(pl.multiple_of(2 * index, 2), 2)

    def cols(index):
        return pl.ds(pl.multiple_of(index * block, block), block)

    def send_rows(d):
        z_, _, to = zc_peer(d)
        send(nrm.at[0:2, cols(z_)], tn.at[pair(zc), :], sent.at[1], got.at[1], to)

    def send_raw(d):
        z_, _, to = zc_peer(d)
        send(tokens.at[:, cols(z_)], tr.at[pair(zc), :], sent.at[2], got.at[2], to)
        send(meta_own.at[0:2, :], meta.at[y, pair(zc), :], sent.at[3], got.at[3], to)

    def half_of(index):
        return nrmh.at[(index * rows) // lanes, 0:2, :]

    def send_halves(d):
        other, to = yc_peer(d)
        send(half_of(other), tny.at[pair(yc), :], sent.at[16], got.at[16], to)

    def z_peer(d):
        return device((z + d) % nz, y, c, x)

    mine_p, mine_o = wqk.at[own, :], wot.at[own, :]
    mine_v, mine_d = wv.at[z, dense_rows, :], wd.at[z, dense_rows, :]
    each(NY, lambda d: send(mine_p, mine_p, sent.at[0], got.at[0], y_peer(d)))
    each(nz, lambda d: send(mine_v, mine_v, sent.at[17], got.at[17], z_peer(d)))
    each(nzc, send_rows)
    each(nyc, send_halves)
    each(NY, lambda d: send(mine_o, mine_o, sent.at[4], got.at[4], y_peer(d)))
    each(nzc, send_raw)
    each(
        nz,
        lambda d: send(
            mine_d,
            mine_d,
            sent.at[5],
            got.at[5],
            z_peer(d),
        ),
    )
    keep_v = pltpu.make_async_copy(half_of(yc), tny.at[pair(yc), :], loads.at[3])
    keep_v.start()
    keep_n = pltpu.make_async_copy(nrm.at[0:2, cols(z)], tn.at[pair(zc), :], loads.at[4])
    keep_r = pltpu.make_async_copy(tokens.at[:, cols(z)], tr.at[pair(zc), :], loads.at[7])
    keep_m = pltpu.make_async_copy(meta_own.at[0:2, :], meta.at[y, pair(zc), :], loads.at[6])
    for copy in (keep_n, keep_r, keep_m):
        copy.start()

    loaded("w_in", "w_forget", "forget_bias", "state_m")
    head_count = state_m.shape[1]
    gate_all = mm(nrm[...], w_in[...], NT)[0:2]
    raw = mm(nrm[...], w_forget[...], NT)[0:2] + forget_bias[...]
    forget_all = jnp.minimum(raw, 0.0) - jnp.log1p(jnp.exp(-jnp.abs(raw)))
    head_lane = iota(gate_all.shape, 1)

    def of_head(values, h):
        mine = head_lane == x * head_count + h
        return jnp.sum(jnp.where(mine, values, 0.0), axis=1, keepdims=True)

    decays, inflows, ms = [], [], []
    for h in range(head_count):
        gate_h, forget_h = of_head(gate_all, h), of_head(forget_all, h)
        kept = forget_h + state_m[:, h : h + 1]
        m_h = jnp.maximum(kept, gate_h)
        decays.append(jnp.exp(kept - m_h))
        inflows.append(jnp.exp(gate_h - m_h))
        ms.append(m_h)
    m_lane = iota(state_m.shape, 1)
    new_m_value = jnp.zeros(state_m.shape, F32)
    for h in range(head_count):
        new_m_value = jnp.where(m_lane == h, ms[h], new_m_value)
    new_m[...] = new_m_value

    keep_n.wait()
    wait_for(count.at[0 : nzc - 1, :, 0:block], got.at[1])
    wait_for(wqk.at[0 : (NY - 1) * rows, :], got.at[0])
    pb[...] = mm(tn[...], wqk[...]).astype(BF)
    keep_p = pltpu.make_async_copy(pb.at[pair(zc), :], rb.at[pair(zc), :], loads.at[4])
    keep_p.start()

    def send_partial(d):
        _, other, to = zc_peer(d)
        send(pb.at[pair(other), :], rb.at[pair(zc), :], sent.at[7], got.at[7], to)

    each(nzc, send_partial)
    keep_v.wait()
    wait_for(count.at[0 : nyc - 1, :, 0 : nz * lanes], got.at[16])
    wait_for(wv.at[0 : nz - 1, 0:rows, :], got.at[17])
    pbv[...] = mm(tny[...], wv[...].reshape(nz * lanes, -1)).astype(BF)
    keep_v = pltpu.make_async_copy(pbv.at[pair(yc), :], rbv.at[pair(yc), :], loads.at[3])
    keep_v.start()

    def send_partial_v(d):
        other, to = yc_peer(d)
        send(pbv.at[pair(other), :], rbv.at[pair(yc), :], sent.at[18], got.at[18], to)

    each(nyc, send_partial_v)
    keep_m.wait()
    wait_for(count.at[0 : nzc - 1, :, 0:128], got.at[3])
    each(NY, lambda d: send(meta.at[y], meta.at[y], sent.at[6], got.at[6], y_peer(d)))

    loaded("state_c", "state_n")
    keep_p.wait()
    wait_for(count.at[0 : nzc - 1, :, 0 : 2 * qk], got.at[7])
    keep_v.wait()
    wait_for(count.at[0 : nyc - 1, :, 0 : 2 * qk], got.at[18])

    def pair_sum(count):
        r, col = iota((16, 2 * count), 0), iota((16, 2 * count), 1)
        return ones_where((col & 1) == r)

    rows_qk = mm(pair_sum(nzc), rb[...]).astype(BF)
    rows_v = mm(pair_sum(nyc), rbv[...]).astype(BF)

    row = iota((16, 1), 0)
    dqk, dv = c_in.shape[2], c_in.shape[3]
    for h in range(head_count):
        q = rows_qk[:, h * dqk : (h + 1) * dqk]
        k = rows_qk[:, qk + h * dqk : qk + (h + 1) * dqk]
        v = rows_v[:, h * dv : (h + 1) * dv]
        qf, kf = q.astype(F32), k.astype(F32)
        heads = jnp.zeros((16, dv), F32)
        for t in range(2):
            decay = decays[h][t : t + 1, :]
            inflow = inflows[h][t : t + 1, :] * dqk ** (-0.5)
            outer = mm(jnp.where(row == t, kf, 0.0).astype(BF), v, TN)
            c_new = decay * c_in[t, h] + inflow * outer
            c_out[t, h] = c_new
            n_new = decay * state_n[t, h : h + 1, :] + inflow * kf[t : t + 1, :]
            new_n[t, h : h + 1, :] = n_new
            numer = mm(qf, c_new, precision=lax.Precision.HIGHEST)
            denom = jnp.sum(qf[t : t + 1, :] * n_new, axis=-1, keepdims=True)
            denom = jnp.maximum(jnp.abs(denom), 1.0)
            heads = jnp.where(row == t, numer / denom, heads)
        hb[:, h * dv : (h + 1) * dv] = heads.astype(BF)

    store_c = pltpu.make_async_copy(c_out, new_c, loads.at[5])
    store_c.start()

    keep_h = pltpu.make_async_copy(hb.at[0:2, :], hg.at[pair(zc), :], loads.at[4])
    keep_h.start()
    each(
        nzc,
        lambda d: send(
            hb.at[0:2, :], hg.at[pair(zc), :], sent.at[8], got.at[8], zc_peer(d)[2]
        ),
    )
    wait_for(wot.at[0 : (NY - 1) * rows, :], got.at[4])
    keep_r.wait()
    wait_for(count.at[0 : nzc - 1, :, 0:block], got.at[2])
    keep_h.wait()
    wait_for(count.at[0 : nzc - 1, :, 0 : 2 * qk], got.at[8])
    op[...] = mm(hg[...], wot[...], NT).astype(BF)
    xc = x * NC + c

    def half_rows(c_):
        return pl.ds(pl.multiple_of(c_ * half, half), half)

    def send_parts(d):
        other = (xc + d) % (n_tp * NC)
        to = device(z, y, other % NC, other // NC)
        send(op.at[half_rows(other % NC), :], og.at[xc], sent.at[9], got.at[9], to)

    each(n_tp * NC, send_parts)
    og[xc] = op[half_rows(c), :]
    wait_for(og.at[0 : n_tp * NC - 1], got.at[9])
    parts = jnp.zeros((half, block), F32)
    for k in range(n_tp * NC):
        parts = parts + og[k].astype(F32)

    sa = z + c * (y - z)
    sb = y + c * (z - y)

    def at(a, b):
        return device(a + c * (b - a), b + c * (a - b), c, x)

    ag[c, sa, sb] = (tr[half_rows(c), :].astype(F32) + parts).astype(BF)
    mine = ag.at[c, sa, sb]
    partner = device(z, y, 1 - c, x)
    near = 2 * min(2, (NY - 1) // 2)
    ring = sorted(range(1, NY), key=lambda d: min(d, NY - d))

    def spread(ref, r):
        for d in sorted(range(1, nz), key=lambda d: -min(d, nz - d)):
            send(ref, ref, sent.at[11], r.at[d], at((sa + d) % nz, sb))

    for d in ring:
        send(mine, mine, sent.at[10], got_y.at[d], at(sa, (sb + d) % NY))
    spread(mine, got_z)
    for index, d in enumerate(ring):
        block_in = ag.at[c, sa, (sb + NY - d) % NY]
        wait_for(block_in, got_y.at[d])
        spread(block_in, got_z if index < near else got_far)

    def swap(ref):
        send(ref, ref, sent.at[12], got.at[11], partner)

    swap(ag.at[c, sa])
    lines = sorted(range(1, nz), key=lambda d: min(d, nz - d))
    for d in lines:
        wait_for(ag.at[0, 0, 0 : near + 1], got_z.at[d])
        wait_for(ag.at[0, 0, near + 1 : NY], got_far.at[d])
        swap(ag.at[c, (sa + nz - d) % nz])
    wait_for(meta.at[0 : NY - 1], got.at[6])
    loaded("moe_gain", "w_group", "w_dense_gate", "w_gate", "w_up", "w_down")
    side = seqs // 2

    def rows_of(h, b):
        pieces = [ag[h, b + h * (k - b), k + h * (b - k)] for k in range(NY)]
        return jnp.concatenate(pieces, axis=0)

    expert = ep.astype(F32)

    def run_half(h):
        squares = jnp.zeros((side, block), F32)
        for b in range(nz):
            piece = rows_of(h, b).astype(F32)
            squares = squares + piece * piece
        mean = jnp.sum(squares, axis=-1, keepdims=True) * (1.0 / width)
        inverse = lax.rsqrt(mean + eps)
        at_rows = pl.ds(pl.multiple_of(h * side, side), side)
        for b in range(nz):
            piece = rows_of(h, b).astype(F32)
            gain = moe_gain[:, b * block : (b + 1) * block]
            n2[at_rows, b * block : (b + 1) * block] = (piece * inverse * gain).astype(BF)
        gate_act = mm(n2[at_rows, :], wg[...])
        up_act = mm(n2[at_rows, :], wu[...])
        act = gate_act * jax.nn.sigmoid(gate_act) * up_act
        facts = meta[:, half_rows(h), :].reshape(side, 128)
        meta_rows[at_rows, :] = facts
        ids = facts.astype(F32)
        assigned = (ids[:, 0:1] == expert) | (ids[:, 1:2] == expert)
        hidden[at_rows, :] = jnp.where(assigned, act, 0.0).astype(BF)

    run_half(c)
    wait_for(ag.at[0], got.at[11])
    run_half(1 - c)

    def token_of(shape):
        r = iota(shape, 1)
        h, y_, rest = r // side, (r // half) % NY, r % half
        z_ = h * (nz // 2) + rest // (2 * NC)
        return ((z_ * NY + y_) * NC) * 2 + rest % (2 * NC)

    slot_rows = iota((n_ep, seqs), 0)
    placing = ones_where(token_of((n_ep, seqs)) // 2 == slot_rows)
    slots = mm(placing, hidden[...]).astype(BF)

    def down(x_):
        return mm(slots, wdn[:, pl.ds(pl.multiple_of(x_ * share, share), share)]).astype(BF)

    for d in range(1, n_tp):
        dp[d] = down((x + d) % n_tp)
    order = sorted(range(nz), key=lambda k: -min(k, nz - k))

    def rows_at(k):
        return pl.ds(pl.multiple_of(((z + k) % nz) * nyc, nyc), nyc)

    for k in order:
        for d in sorted(range(1, n_tp), key=lambda d: -min(d, n_tp - d)):
            to = device(z, y, c, (x + d) % n_tp)
            send(dp.at[d, rows_at(k)], xg.at[x, rows_at(k)], sent.at[13], got_x.at[k], to)
    xg[x] = down(x)

    local = ones_where(token_of((2 * nyc, seqs)) == z * 2 * nyc + iota((2 * nyc, seqs), 0))
    picks = mm(local, meta_rows[...])
    zrows = mm(local, n2[...]).astype(BF)
    n2z[...] = zrows
    wait_for(wd.at[0 : nz - 1, 0:rows, :], got.at[5])
    dense = jnp.zeros((2 * nyc, share), F32)
    for b in range(nz):
        at_lane = pl.multiple_of(b * block + dense_block * lanes, lanes)
        dense = dense + mm(n2z[:, pl.ds(at_lane, lanes)], wd[b])
    gate_rows = w_dense_gate[...].astype(F32)
    products = jnp.zeros((2 * nyc, 128), F32)
    for k in range(width // 128):
        at_cols = slice(k * 128, (k + 1) * 128)
        products = products + zrows[:, at_cols].astype(F32) * gate_rows[k : k + 1, :]
    dense_gate = jnp.sum(products, axis=-1, keepdims=True)
    dense = jax.nn.sigmoid(dense_gate) * dense
    logits = mm(zrows, w_group[...], NT)
    shifted = jnp.exp(logits - jnp.max(logits, axis=-1, keepdims=True))
    prob = shifted / jnp.sum(shifted, axis=-1, keepdims=True)
    per_group = n_ep // group_count
    first = (iota(prob.shape, 1) * per_group).astype(F32)
    weights = [picks[:, 2 + j : 3 + j] + picks[:, 4 + j : 5 + j] for j in range(2)]
    total = weights[0] + weights[1]
    at_slot = iota((2 * nyc, n_ep), 1)
    source = ((at_slot // nyc) * nyc + yc).astype(F32)
    same = at_slot % nyc == iota((2 * nyc, n_ep), 0) // 2
    mixing = jnp.zeros((2 * nyc, n_ep), F32)
    for j in range(2):
        ident = picks[:, j : j + 1]
        member = (ident >= first) & (ident < first + per_group)
        picked = jnp.sum(jnp.where(member, prob, 0.0), axis=-1, keepdims=True)
        route = picked * weights[j] / total
        mixing = mixing + jnp.where(same & (ident == source), route, 0.0)
    mix_hi = mixing.astype(BF)
    mix_lo = (mixing - mix_hi.astype(F32)).astype(BF)
    owned = ones_where(
        (token_of((16, seqs)) == 2 * ep + iota((16, seqs), 0)) & (iota((16, seqs), 0) < 2)
    )
    per_share = nz // n_tp
    residual = []
    for k in range(per_share):
        b = x * per_share + k
        residual.append(
            mm(owned[:, 0:side], ag[0, b].reshape(side, block))
            + mm(owned[:, side:], ag[1, :, b].reshape(side, block))
        )

    for k in order:
        wait_for(xg.at[0 : n_tp - 1, 0:nyc, :], got_x.at[k])
        total_out = xg[0, rows_at(k), :].astype(F32)
        for j in range(1, n_tp):
            total_out = total_out + xg[j, rows_at(k), :].astype(F32)
        if k == 0:
            zg[z] = total_out.astype(BF)
        else:
            eo[rows_at(k), :] = total_out.astype(BF)
            send(eo.at[rows_at(k), :], zg.at[z], sent.at[14], got.at[13], z_peer(k))
    wait_for(zg.at[0 : nz - 1], got.at[13])
    arrived = zg[...].reshape(n_ep, share)
    ys[...] = (mm(mix_hi, arrived) + mm(mix_lo, arrived) + dense).astype(BF)
    keep_y = pltpu.make_async_copy(ys.at[pair(yc), :], yg.at[pair(yc), :], loads.at[4])
    keep_y.start()

    def send_sums(d):
        other, to = yc_peer(d)
        send(ys.at[pair(other), :], yg.at[pair(yc), :], sent.at[15], got.at[14], to)

    each(nyc, send_sums)
    keep_y.wait()
    wait_for(count.at[0 : nyc - 1, :, 0:share], got.at[14])
    summed = mm(pair_sum(nyc), yg[...])
    for k in range(per_share):
        at_cols = slice(k * block, (k + 1) * block)
        mixed[:, at_cols] = (residual[k] + summed[:, at_cols])[0:2].astype(BF)

    store_c.wait()
    wait_for(wqk.at[0 : (NY - 1) * rows, :], sent.at[0])
    wait_for(count.at[0 : nyc - 1, :, 0 : nz * lanes], sent.at[16])
    wait_for(wv.at[0 : nz - 1, 0:rows, :], sent.at[17])
    wait_for(count.at[0 : nyc - 1, :, 0 : 2 * qk], sent.at[18])
    wait_for(count.at[0 : nzc - 1, :, 0:block], sent.at[1])
    wait_for(count.at[0 : nzc - 1, :, 0:block], sent.at[2])
    wait_for(count.at[0 : nzc - 1, :, 0:128], sent.at[3])
    wait_for(wot.at[0 : (NY - 1) * rows, :], sent.at[4])
    wait_for(wd.at[0 : nz - 1, 0:rows, :], sent.at[5])
    wait_for(meta.at[0 : NY - 1], sent.at[6])
    wait_for(count.at[0 : nzc - 1, :, 0 : 2 * qk], sent.at[7])
    wait_for(count.at[0 : nzc - 1, :, 0 : 2 * qk], sent.at[8])
    wait_for(og.at[0 : n_tp * NC - 1], sent.at[9])
    wait_for(ag.at[0, 0, 0 : NY - 1], sent.at[10])
    wait_for(ag.at[0, 0 : nz - 1], sent.at[11])
    wait_for(ag.at[0], sent.at[12])
    wait_for(xg.at[0 : n_tp - 1], sent.at[13])
    wait_for(zg.at[0 : nz - 1], sent.at[14])
    wait_for(count.at[0 : nyc - 1, :, 0:share], sent.at[15])


def per_device(
    tokens,
    state_c,
    state_n,
    state_m,
    mix_gain,
    w_query,
    w_key,
    w_value,
    w_input_gate,
    w_forget_gate,
    forget_bias,
    w_output,
    moe_gain,
    w_group,
    expert_ids,
    expert_weight,
    w_exp_gate,
    w_exp_up,
    w_exp_down,
    w_dense,
    w_dense_gate,
):
    n_ep, n_tp = lax.axis_size("ep"), lax.axis_size("tp")
    nz = n_ep // (NY * NC)
    width = tokens.shape[1]
    rows = w_query.shape[0]
    block = NY * NC * rows
    lanes = min(128, block)
    share = width // n_tp
    nzc, nyc = nz * NC, NY * NC
    hidden = w_exp_gate.shape[2]
    qkv = 2 * w_query.shape[1] + w_value.shape[1]
    vm = pl.BlockSpec(memory_space=pltpu.VMEM)
    anywhere = pl.BlockSpec(memory_space=pltpu.HBM)
    V = pltpu.VMEM

    def kernel(*refs):
        layer_kernel(n_ep, n_tp, *refs)

    in_specs = [anywhere] * 21
    out_shape = (
        jax.ShapeDtypeStruct((2, share), BF),
        jax.ShapeDtypeStruct(state_c.shape, F32),
        jax.ShapeDtypeStruct(state_n.shape, F32),
        jax.ShapeDtypeStruct(state_m.shape, F32),
    )
    scratch = [
        V((16, width), BF),
        V((block // lanes, 16, nz * lanes), BF),
        V((2 * nzc, block), BF),
        V((2 * nyc, nz * lanes), BF),
        V((2 * nzc, block), BF),
        V((16, 128), BF),
        V((NY, 2 * nzc, 128), BF),
        V((block, 2 * w_query.shape[1]), BF),
        V((nz, lanes, w_value.shape[1]), BF),
        V((block, w_output.shape[0]), BF),
        V((nz, lanes, share), BF),
        V((2 * nzc, 2 * w_query.shape[1]), BF),
        V((2 * nzc, 2 * w_query.shape[1]), BF),
        V((2 * nyc, w_value.shape[1]), BF),
        V((2 * nyc, w_value.shape[1]), BF),
        V(state_c.shape, F32),
        V(state_c.shape, F32),
        V((16, w_output.shape[0]), BF),
        V((2 * nzc, w_output.shape[0]), BF),
        V((2 * nzc, block), BF),
        V((n_tp * NC, nzc, block), BF),
        V((2, nz, NY, nzc, block), BF),
        V((2 * n_ep, width), BF),
        V((2 * n_ep, hidden), BF),
        V((2 * n_ep, 128), BF),
        V((2 * nyc, width), BF),
        V((width, hidden), BF),
        V((width, hidden), BF),
        V((hidden, width), BF),
        V((n_tp, n_ep, share), BF),
        V((n_tp, n_ep, share), BF),
        V((n_ep, share), BF),
        V((nz, nyc, share), BF),
        V((2 * nyc, share), BF),
        V((2 * nyc, share), BF),
        pltpu.SemaphoreType.DMA((32,)),
        pltpu.SemaphoreType.DMA((20,)),
        pltpu.SemaphoreType.DMA((20,)),
        pltpu.SemaphoreType.DMA((nz,)),
        pltpu.SemaphoreType.DMA((nz,)),
        pltpu.SemaphoreType.DMA((NY,)),
        pltpu.SemaphoreType.DMA((nz,)),
        V((max(nzc, nyc), 2, qkv), BF),
        V(tokens.shape, BF),
        V(state_n.shape, F32),
        V(state_m.shape, F32),
        V((1, width), F32),
        V(w_input_gate.shape[::-1], BF),
        V(w_forget_gate.shape[::-1], BF),
        V((1, forget_bias.shape[0]), F32),
        V((1, width), F32),
        V(w_group.shape[::-1], BF),
        V(expert_ids.shape, jnp.int32),
        V(expert_weight.shape, F32),
        V((width // 128, 128), BF),
    ]
    results = pl.pallas_call(
        kernel,
        name="layer",
        out_shape=out_shape,
        in_specs=in_specs,
        out_specs=(vm, anywhere, vm, vm),
        scratch_shapes=scratch,
        compiler_params=pltpu.CompilerParams(
            collective_id=0, has_side_effects=True, vmem_limit_bytes=67043328
        ),
    )(
        tokens,
        state_c,
        state_n,
        state_m,
        mix_gain.reshape(1, -1),
        w_query,
        w_key,
        w_value,
        w_input_gate.T,
        w_forget_gate.T,
        forget_bias.reshape(1, -1),
        w_output.T,
        moe_gain.reshape(1, -1),
        w_group.T,
        expert_ids,
        expert_weight,
        w_exp_gate,
        w_exp_up,
        w_exp_down,
        w_dense,
        w_dense_gate.reshape(-1, 128),
    )
    return pl.pallas_call(
        store_kernel,
        name="store",
        out_shape=out_shape,
        in_specs=[anywhere] * 4,
        out_specs=(anywhere,) * 4,
        scratch_shapes=[V(r.shape, r.dtype) for r in out_shape] + [pltpu.SemaphoreType.DMA((2, 4))],
        compiler_params=pltpu.CompilerParams(vmem_limit_bytes=67043328),
    )(*results)


def store_kernel(*refs):
    ins, outs, held, sems = refs[0:4], refs[4:8], refs[8:12], refs[12]
    order = (1, 0, 2, 3)
    for k in order:
        pltpu.make_async_copy(ins[k], held[k], sems.at[0, k]).start()
    for k in order:
        pltpu.make_async_copy(ins[k], held[k], sems.at[0, k]).wait()
        pltpu.make_async_copy(held[k], outs[k], sems.at[1, k]).start()
    for k in order:
        pltpu.make_async_copy(held[k], outs[k], sems.at[1, k]).wait()


def solution(mesh):
    placed = (
        P("ep", None),
        P("ep", "tp", None, None),
        P("ep", "tp", None),
        P("ep", "tp"),
        P(),
        P("ep", "tp"),
        P("ep", "tp"),
        P("ep", "tp"),
        P(),
        P(),
        P(),
        P("tp", "ep"),
        P(),
        P(),
        P("ep", None),
        P("ep", None),
        P("ep", None, "tp"),
        P("ep", None, "tp"),
        P("ep", "tp", None),
        P("ep", "tp"),
        P(),
    )
    return jax.shard_map(
        per_device,
        mesh=mesh,
        in_specs=placed,
        out_specs=(P("ep", "tp"), P("ep", "tp", None, None), P("ep", "tp", None), P("ep", "tp")),
        check_vma=False,
    )
```

```python
import jax
import jax.numpy as jnp
from jax import lax
from jax.experimental import pallas as pl
from jax.experimental.pallas import tpu as pltpu
from jax.sharding import PartitionSpec as P

NY = 8
NC = 2
eps = 1e-06
BF = jnp.bfloat16
F32 = jnp.float32
MESH = pl.DeviceIdType.MESH
NN = (((1,), (0,)), ((), ()))
NT = (((1,), (1,)), ((), ()))
TN = (((0,), (0,)), ((), ()))


def mm(a, b, dims=NN, precision=None):
    return lax.dot_general(a, b, dims, precision=precision, preferred_element_type=F32)


def iota(shape, dim):
    return lax.broadcasted_iota(jnp.int32, shape, dim)


def ones_where(mask):
    return jnp.where(mask, 1.0, 0.0).astype(BF)


def each(count, body):
    def step(i, carry):
        away = lax.div(i + 1, 2)
        body(count // 2 + away - 2 * lax.rem(i, 2) * away)
        return carry

    lax.fori_loop(0, count - 1, step, 0)


def wait_for(ref, sem):
    pltpu.make_async_copy(ref, ref, sem).wait()


def layer_kernel(
    n_ep,
    n_tp,
    tokens_h,
    state_c_h,
    state_n_h,
    state_m_h,
    mix_gain_h,
    w_query_h,
    w_key_h,
    w_value_h,
    w_in_h,
    w_forget_h,
    forget_bias_h,
    w_out_h,
    moe_gain_h,
    w_group_h,
    expert_ids_h,
    expert_weight_h,
    w_gate_h,
    w_up_h,
    w_down_h,
    w_dense_h,
    w_dense_gate_h,
    mixed,
    new_c,
    new_n,
    new_m,
    nrm,
    nrmh,
    tn,
    tny,
    tr,
    meta_own,
    meta,
    wqk,
    wv,
    wot,
    wd,
    pb,
    rb,
    pbv,
    rbv,
    c_in,
    c_out,
    n_out,
    m_out,
    mixed_out,
    hb,
    hg,
    op,
    og,
    ag,
    n2,
    meta_rows,
    n2z,
    wg,
    wu,
    wdn,
    dp,
    xg,
    eo,
    zg,
    ys,
    yg,
    loads,
    sent,
    got,
    got_z,
    got_far,
    got_y,
    got_x,
    count,
    tokens,
    state_n,
    state_m,
    mix_gain,
    w_in,
    w_forget,
    forget_bias,
    moe_gain,
    w_group,
    expert_ids,
    expert_weight,
    w_dense_gate,
):
    nz = n_ep // (NY * NC)
    rows = w_query_h.shape[0]
    width = tokens.shape[1]
    block = NY * NC * rows
    nzc, nyc = nz * NC, NY * NC
    half = nz * NC
    seqs = 2 * n_ep
    share = width // n_tp
    qk = w_query_h.shape[1]
    lanes = wd.shape[1]
    group_count = w_group.shape[0]

    ep = lax.axis_index("ep")
    x = lax.axis_index("tp")
    z = lax.div(ep, nyc)
    y = lax.rem(lax.div(ep, NC), NY)
    c = lax.rem(ep, NC)
    zc = z * NC + c
    yc = y * NC + c

    def device(z_, y_, c_, x_):
        return {"ep": (z_ * NY + y_) * NC + c_, "tp": x_}

    def send(src, dst, s, r, to):
        pltpu.make_async_remote_copy(
            src_ref=src, dst_ref=dst, send_sem=s, recv_sem=r, device_id=to, device_id_type=MESH
        ).start()

    def y_peer(d):
        return device(z, lax.rem(y + d, NY), c, x)

    def zc_peer(d):
        other = lax.rem(zc + d, nzc)
        z_ = lax.div(other, NC)
        return z_, other, device(z_, y, lax.rem(other, NC), x)

    def yc_peer(d):
        other = lax.rem(yc + d, nyc)
        return other, {"ep": z * nyc + other, "tp": x}

    def xc_peer(d):
        other = lax.rem(x * NC + c + d, n_tp * NC)
        return device(z, y, lax.rem(other, NC), lax.div(other, NC))

    wqk[...] = jnp.zeros_like(wqk)
    wv[...] = jnp.zeros_like(wv)
    wot[...] = jnp.zeros_like(wot)
    wd[...] = jnp.zeros_like(wd)

    barrier = pltpu.get_barrier_semaphore()

    def greet(to):
        pl.semaphore_signal(barrier, inc=1, device_id=to, device_id_type=MESH)

    each(nyc, lambda d: greet(yc_peer(d)[1]))
    each(nzc, lambda d: greet(zc_peer(d)[2]))
    each(n_tp, lambda d: greet(device(z, y, c, lax.rem(x + d, n_tp))))

    started = {}

    def load(name, src, dst):
        started[name] = pltpu.make_async_copy(src, dst, loads.at[8 + len(started)])
        started[name].start()

    load("tokens", tokens_h, tokens)
    load("mix_gain", mix_gain_h, mix_gain)
    load("expert_ids", expert_ids_h, expert_ids)
    load("expert_weight", expert_weight_h, expert_weight)
    own = pl.ds(pl.multiple_of(yc * rows, rows), rows)
    start = yc * rows
    dense_block = start // lanes
    dense_rows = pl.ds(pl.multiple_of(start % lanes, rows), rows)
    load("w_query", w_query_h, wqk.at[own, 0:qk])
    load("w_key", w_key_h, wqk.at[own, qk : 2 * qk])
    load("w_value", w_value_h, wv.at[z, dense_rows, :])
    load("w_out", w_out_h, wot.at[own, :])
    load("w_dense", w_dense_h, wd.at[z, dense_rows, :])
    load("w_in", w_in_h, w_in)
    load("w_forget", w_forget_h, w_forget)
    load("forget_bias", forget_bias_h, forget_bias)
    load("state_m", state_m_h, state_m)
    load("state_n", state_n_h, state_n)
    load("state_c", state_c_h, c_in)
    load("moe_gain", moe_gain_h, moe_gain)
    load("w_group", w_group_h, w_group)
    load("w_dense_gate", w_dense_gate_h, w_dense_gate)
    load("w_gate", w_gate_h.at[0], wg)
    load("w_up", w_up_h.at[0], wu)
    load("w_down", w_down_h.at[0], wdn)

    def loaded(*names):
        for name in names:
            started[name].wait()

    loaded("tokens", "mix_gain", "expert_ids", "expert_weight")
    wide = tokens[...].astype(F32)
    inverse = lax.rsqrt(jnp.mean(wide * wide, axis=-1, keepdims=True) + eps)
    nrm[...] = jnp.zeros_like(nrm)
    normed = (wide * inverse * mix_gain[...]).astype(BF)
    nrm[0:2, :] = normed
    for k in range(block // lanes):
        for b in range(nz):
            first = b * block + k * lanes
            nrmh[k, 0:2, b * lanes : (b + 1) * lanes] = normed[:, first : first + lanes]
    lane = iota((2, 128), 1)
    idf = expert_ids[...].astype(F32)
    ewt = expert_weight[...]
    ew_hi = ewt.astype(BF).astype(F32)
    ew_lo = ewt - ew_hi
    packed = jnp.zeros((2, 128), F32)
    for k, part in enumerate((idf, ew_hi, ew_lo)):
        for j in range(2):
            packed = jnp.where(lane == 2 * k + j, part[:, j : j + 1], packed)
    meta_own[...] = jnp.zeros_like(meta_own)
    meta_own[0:2, :] = packed.astype(BF)

    loaded("w_query", "w_key", "w_value", "w_out", "w_dense")
    pl.semaphore_wait(barrier, (nyc - 1) + (nzc - 1) + (n_tp - 1))

    def pair(index):
        return pl.ds(pl.multiple_of(2 * index, 2), 2)

    def cols(index):
        return pl.ds(pl.multiple_of(index * block, block), block)

    def send_rows(d):
        z_, _, to = zc_peer(d)
        send(nrm.at[0:2, cols(z_)], tn.at[pair(zc), :], sent.at[1], got.at[1], to)

    def send_raw(d):
        z_, _, to = zc_peer(d)
        send(tokens.at[:, cols(z_)], tr.at[pair(zc), :], sent.at[2], got.at[2], to)
        send(meta_own.at[0:2, :], meta.at[y, pair(zc), :], sent.at[3], got.at[3], to)

    def half_of(index):
        return nrmh.at[lax.div(index * rows, lanes), 0:2, :]

    def send_halves(d):
        other, to = yc_peer(d)
        send(half_of(other), tny.at[pair(yc), :], sent.at[16], got.at[16], to)

    def z_peer(d):
        return device(lax.rem(z + d, nz), y, c, x)

    mine_p, mine_o = wqk.at[own, :], wot.at[own, :]
    mine_v, mine_d = wv.at[z, dense_rows, :], wd.at[z, dense_rows, :]
    each(NY, lambda d: send(mine_p, mine_p, sent.at[0], got.at[0], y_peer(d)))
    each(nz, lambda d: send(mine_v, mine_v, sent.at[17], got.at[17], z_peer(d)))
    each(nzc, send_rows)
    each(nyc, send_halves)
    each(NY, lambda d: send(mine_o, mine_o, sent.at[4], got.at[4], y_peer(d)))
    each(nzc, send_raw)
    each(
        nz,
        lambda d: send(
            mine_d,
            mine_d,
            sent.at[5],
            got.at[5],
            z_peer(d),
        ),
    )
    keep_v = pltpu.make_async_copy(half_of(yc), tny.at[pair(yc), :], loads.at[3])
    keep_v.start()
    keep_n = pltpu.make_async_copy(nrm.at[0:2, cols(z)], tn.at[pair(zc), :], loads.at[4])
    keep_r = pltpu.make_async_copy(tokens.at[:, cols(z)], tr.at[pair(zc), :], loads.at[7])
    keep_m = pltpu.make_async_copy(meta_own.at[0:2, :], meta.at[y, pair(zc), :], loads.at[6])
    for copy in (keep_n, keep_r, keep_m):
        copy.start()

    loaded("w_in", "w_forget", "forget_bias", "state_m")
    head_count = state_m.shape[1]
    gate_all = mm(nrm[...], w_in[...], NT)[0:2]
    raw = mm(nrm[...], w_forget[...], NT)[0:2] + forget_bias[...]
    forget_all = jnp.minimum(raw, 0.0) - jnp.log1p(jnp.exp(-jnp.abs(raw)))
    head_lane = iota(gate_all.shape, 1)

    def of_head(values, h):
        mine = head_lane == x * head_count + h
        return jnp.sum(jnp.where(mine, values, 0.0), axis=1, keepdims=True)

    decays, inflows, ms = [], [], []
    for h in range(head_count):
        gate_h, forget_h = of_head(gate_all, h), of_head(forget_all, h)
        kept = forget_h + state_m[:, h : h + 1]
        m_h = jnp.maximum(kept, gate_h)
        decays.append(jnp.exp(kept - m_h))
        inflows.append(jnp.exp(gate_h - m_h))
        ms.append(m_h)
    m_lane = iota(state_m.shape, 1)
    new_m_value = jnp.zeros(state_m.shape, F32)
    for h in range(head_count):
        new_m_value = jnp.where(m_lane == h, ms[h], new_m_value)
    m_out[...] = new_m_value
    store_m = pltpu.make_async_copy(m_out, new_m, loads.at[1])
    store_m.start()

    keep_n.wait()
    wait_for(count.at[0 : nzc - 1, :, 0:block], got.at[1])
    wait_for(wqk.at[0 : (NY - 1) * rows, :], got.at[0])
    pb[...] = mm(tn[...], wqk[...]).astype(BF)
    keep_p = pltpu.make_async_copy(pb.at[pair(zc), :], rb.at[pair(zc), :], loads.at[4])
    keep_p.start()

    def send_partial(d):
        _, other, to = zc_peer(d)
        send(pb.at[pair(other), :], rb.at[pair(zc), :], sent.at[7], got.at[7], to)

    each(nzc, send_partial)
    keep_v.wait()
    wait_for(count.at[0 : nyc - 1, :, 0 : nz * lanes], got.at[16])
    wait_for(wv.at[0 : nz - 1, 0:rows, :], got.at[17])
    pbv[...] = mm(tny[...], wv[...].reshape(nz * lanes, -1)).astype(BF)
    keep_v = pltpu.make_async_copy(pbv.at[pair(yc), :], rbv.at[pair(yc), :], loads.at[3])
    keep_v.start()

    def send_partial_v(d):
        other, to = yc_peer(d)
        send(pbv.at[pair(other), :], rbv.at[pair(yc), :], sent.at[18], got.at[18], to)

    each(nyc, send_partial_v)
    keep_m.wait()
    wait_for(count.at[0 : nzc - 1, :, 0:128], got.at[3])
    each(NY, lambda d: send(meta.at[y], meta.at[y], sent.at[6], got.at[6], y_peer(d)))

    loaded("state_c", "state_n")
    keep_p.wait()
    wait_for(count.at[0 : nzc - 1, :, 0 : 2 * qk], got.at[7])
    keep_v.wait()
    wait_for(count.at[0 : nyc - 1, :, 0 : 2 * qk], got.at[18])

    def pair_sum(count):
        r, col = iota((16, 2 * count), 0), iota((16, 2 * count), 1)
        return ones_where((col & 1) == r)

    rows_qk = mm(pair_sum(nzc), rb[...]).astype(BF)
    rows_v = mm(pair_sum(nyc), rbv[...]).astype(BF)

    row = iota((16, 1), 0)
    dqk, dv = c_in.shape[2], c_in.shape[3]
    for h in range(head_count):
        q = rows_qk[:, h * dqk : (h + 1) * dqk]
        k = rows_qk[:, qk + h * dqk : qk + (h + 1) * dqk]
        v = rows_v[:, h * dv : (h + 1) * dv]
        qf, kf = q.astype(F32), k.astype(F32)
        heads = jnp.zeros((16, dv), F32)
        for t in range(2):
            decay = decays[h][t : t + 1, :]
            inflow = inflows[h][t : t + 1, :] * dqk ** (-0.5)
            outer = mm(jnp.where(row == t, kf, 0.0).astype(BF), v, TN)
            c_new = decay * c_in[t, h] + inflow * outer
            c_out[t, h] = c_new
            n_new = decay * state_n[t, h : h + 1, :] + inflow * kf[t : t + 1, :]
            n_out[t, h : h + 1, :] = n_new
            numer = mm(qf, c_new, precision=lax.Precision.HIGHEST)
            denom = jnp.sum(qf[t : t + 1, :] * n_new, axis=-1, keepdims=True)
            denom = jnp.maximum(jnp.abs(denom), 1.0)
            heads = jnp.where(row == t, numer / denom, heads)
        hb[:, h * dv : (h + 1) * dv] = heads.astype(BF)

    store_c = pltpu.make_async_copy(c_out, new_c, loads.at[5])
    store_c.start()
    store_n = pltpu.make_async_copy(n_out, new_n, loads.at[2])
    store_n.start()

    keep_h = pltpu.make_async_copy(hb.at[0:2, :], hg.at[pair(zc), :], loads.at[4])
    keep_h.start()
    each(
        nzc,
        lambda d: send(
            hb.at[0:2, :], hg.at[pair(zc), :], sent.at[8], got.at[8], zc_peer(d)[2]
        ),
    )
    wait_for(wot.at[0 : (NY - 1) * rows, :], got.at[4])
    keep_r.wait()
    wait_for(count.at[0 : nzc - 1, :, 0:block], got.at[2])
    keep_h.wait()
    wait_for(count.at[0 : nzc - 1, :, 0 : 2 * qk], got.at[8])
    op[...] = mm(hg[...], wot[...], NT).astype(BF)
    xc = x * NC + c

    def half_rows(c_):
        return pl.ds(pl.multiple_of(c_ * half, half), half)

    def send_parts(d):
        other = (xc + d) % (n_tp * NC)
        to = device(z, y, other % NC, other // NC)
        send(op.at[half_rows(other % NC), :], og.at[xc], sent.at[9], got.at[9], to)

    each(n_tp * NC, send_parts)
    og[xc] = op[half_rows(c), :]
    wait_for(og.at[0 : n_tp * NC - 1], got.at[9])
    parts = jnp.zeros((half, block), F32)
    for k in range(n_tp * NC):
        parts = parts + og[k].astype(F32)

    sa = z + c * (y - z)
    sb = y + c * (z - y)

    def at(a, b):
        return device(a + c * (b - a), b + c * (a - b), c, x)

    ag[c, sa, sb] = (tr[half_rows(c), :].astype(F32) + parts).astype(BF)
    mine = ag.at[c, sa, sb]
    partner = device(z, y, 1 - c, x)
    near = 2 * min(2, (NY - 1) // 2)
    ring = sorted(range(1, NY), key=lambda d: min(d, NY - d))

    def spread(ref, r):
        for d in sorted(range(1, nz), key=lambda d: -min(d, nz - d)):
            send(ref, ref, sent.at[11], r.at[d], at(lax.rem(sa + d, nz), sb))

    for d in reversed(ring):
        send(mine, mine, sent.at[10], got_y.at[d], at(sa, lax.rem(sb + d, NY)))
    spread(mine, got_z)
    for index, d in enumerate(ring):
        block_in = ag.at[c, sa, lax.rem(sb + NY - d, NY)]
        wait_for(block_in, got_y.at[d])
        spread(block_in, got_z if index < near else got_far)

    def swap(ref):
        send(ref, ref, sent.at[12], got.at[11], partner)

    swap(ag.at[c, sa])
    lines = sorted(range(1, nz), key=lambda d: min(d, nz - d))
    for d in lines:
        wait_for(ag.at[0, 0, 0 : near + 1], got_z.at[d])
        wait_for(ag.at[0, 0, near + 1 : NY], got_far.at[d])
        swap(ag.at[c, lax.rem(sa + nz - d, nz)])
    wait_for(meta.at[0 : NY - 1], got.at[6])
    loaded("moe_gain", "w_group", "w_dense_gate", "w_gate", "w_up", "w_down")
    side = seqs // 2

    def rows_of(h, b):
        pieces = [ag[h, b + h * (k - b), k + h * (b - k)] for k in range(NY)]
        return jnp.concatenate(pieces, axis=0)

    expert = ep.astype(F32)

    local_row = iota((n_ep // 2, side), 1)
    local_slot = (local_row % half) // (2 * NC) * nyc
    local_slot = local_slot + (local_row // half) * NC + (local_row % (2 * NC)) // 2
    placing = ones_where(local_slot == iota((n_ep // 2, side), 0))
    quarter = nz // 2
    order = [0] + sorted(range(1, quarter), key=lambda k: -abs(2 * k - quarter))

    def rows_at(h, j):
        z_ = h * quarter + (z % quarter + j) % quarter
        return z_, pl.ds(pl.multiple_of(z_ * nyc, nyc), nyc)

    def first_or_second(h):
        return (h + c) % 2

    def run_half(h):
        squares = jnp.zeros((side, block), F32)
        for b in range(nz):
            piece = rows_of(h, b).astype(F32)
            squares = squares + piece * piece
        mean = jnp.sum(squares, axis=-1, keepdims=True) * (1.0 / width)
        inverse = lax.rsqrt(mean + eps)
        at_rows = pl.ds(pl.multiple_of(h * side, side), side)
        for b in range(nz):
            piece = rows_of(h, b).astype(F32)
            gain = moe_gain[:, b * block : (b + 1) * block]
            n2[at_rows, b * block : (b + 1) * block] = (piece * inverse * gain).astype(BF)
        gate_act = mm(n2[at_rows, :], wg[...])
        up_act = mm(n2[at_rows, :], wu[...])
        act = gate_act * jax.nn.sigmoid(gate_act) * up_act
        facts = meta[:, half_rows(h), :].reshape(side, 128)
        meta_rows[at_rows, :] = facts
        ids = facts.astype(F32)
        assigned = (ids[:, 0:1] == expert) | (ids[:, 1:2] == expert)
        masked = jnp.where(assigned, act, 0.0).astype(BF)
        slots = mm(placing, masked).astype(BF)
        at_slots = pl.ds(pl.multiple_of(h * (n_ep // 2), n_ep // 2), n_ep // 2)

        def down(x_):
            cut = pl.ds(pl.multiple_of(x_ * share, share), share)
            return mm(slots, wdn[:, cut]).astype(BF)

        for d in range(1, n_tp):
            dp[d, at_slots, :] = down((x + d) % n_tp)
        for j in order:
            at_block = rows_at(h, j)[1]
            for d in sorted(range(1, n_tp), key=lambda d: -min(d, n_tp - d)):
                to = device(z, y, c, (x + d) % n_tp)
                got_b = got_x.at[first_or_second(h) * (nz // 2) + j]
                send(dp.at[d, at_block], xg.at[x, at_block], sent.at[13], got_b, to)
        xg[x, at_slots, :] = down(x)

    run_half(c)
    wait_for(ag.at[0], got.at[11])
    run_half(1 - c)

    def token_of(shape):
        r = iota(shape, 1)
        h, y_, rest = r // side, (r // half) % NY, r % half
        z_ = h * (nz // 2) + rest // (2 * NC)
        return ((z_ * NY + y_) * NC) * 2 + rest % (2 * NC)

    local = ones_where(token_of((2 * nyc, seqs)) == z * 2 * nyc + iota((2 * nyc, seqs), 0))
    picks = mm(local, meta_rows[...])
    zrows = mm(local, n2[...]).astype(BF)
    n2z[...] = zrows
    wait_for(wd.at[0 : nz - 1, 0:rows, :], got.at[5])
    dense = jnp.zeros((2 * nyc, share), F32)
    for b in range(nz):
        at_lane = pl.multiple_of(b * block + dense_block * lanes, lanes)
        dense = dense + mm(n2z[:, pl.ds(at_lane, lanes)], wd[b])
    gate_rows = w_dense_gate[...].astype(F32)
    products = jnp.zeros((2 * nyc, 128), F32)
    for k in range(width // 128):
        at_cols = slice(k * 128, (k + 1) * 128)
        products = products + zrows[:, at_cols].astype(F32) * gate_rows[k : k + 1, :]
    dense_gate = jnp.sum(products, axis=-1, keepdims=True)
    dense = jax.nn.sigmoid(dense_gate) * dense
    logits = mm(zrows, w_group[...], NT)
    shifted = jnp.exp(logits - jnp.max(logits, axis=-1, keepdims=True))
    prob = shifted / jnp.sum(shifted, axis=-1, keepdims=True)
    per_group = n_ep // group_count
    first = (iota(prob.shape, 1) * per_group).astype(F32)
    weights = [picks[:, 2 + j : 3 + j] + picks[:, 4 + j : 5 + j] for j in range(2)]
    total = weights[0] + weights[1]
    at_slot = iota((2 * nyc, n_ep), 1)
    source = ((at_slot // nyc) * nyc + yc).astype(F32)
    same = at_slot % nyc == iota((2 * nyc, n_ep), 0) // 2
    mixing = jnp.zeros((2 * nyc, n_ep), F32)
    for j in range(2):
        ident = picks[:, j : j + 1]
        member = (ident >= first) & (ident < first + per_group)
        picked = jnp.sum(jnp.where(member, prob, 0.0), axis=-1, keepdims=True)
        route = picked * weights[j] / total
        mixing = mixing + jnp.where(same & (ident == source), route, 0.0)
    mix_hi = mixing.astype(BF)
    mix_lo = (mixing - mix_hi.astype(F32)).astype(BF)
    mix_both = jnp.concatenate([mix_hi, mix_lo], axis=1)
    owned = ones_where(
        (token_of((16, seqs)) == 2 * ep + iota((16, seqs), 0)) & (iota((16, seqs), 0) < 2)
    )
    per_share = nz // n_tp
    residual = []
    for k in range(per_share):
        b = x * per_share + k
        residual.append(
            mm(owned[:, 0:side], ag[0, b].reshape(side, block))
            + mm(owned[:, side:], ag[1, :, b].reshape(side, block))
        )

    for turn in range(2):
        for j in order:
            z_, at_block = rows_at((c + turn) % 2, j)
            wait_for(xg.at[0 : n_tp - 1, 0:nyc, :], got_x.at[turn * quarter + j])
            total_out = xg[0, at_block, :].astype(F32)
            for k in range(1, n_tp):
                total_out = total_out + xg[k, at_block, :].astype(F32)
            eo[at_block, :] = total_out.astype(BF)

            def deliver(z_=z_, at_block=at_block):
                send(eo.at[at_block, :], zg.at[z], sent.at[14], got.at[13], device(z_, y, c, x))

            def keep(at_block=at_block):
                zg[z] = eo[at_block, :]

            if j == 0:
                pl.when(z_ != z)(deliver)
                pl.when(z_ == z)(keep)
            else:
                deliver()
    wait_for(zg.at[0 : nz - 1], got.at[13])
    arrived = zg[...].reshape(n_ep, share)
    twice = jnp.concatenate([arrived, arrived], axis=0)
    ys[...] = (mm(mix_both, twice) + dense).astype(BF)
    keep_y = pltpu.make_async_copy(ys.at[pair(yc), :], yg.at[pair(yc), :], loads.at[4])
    keep_y.start()

    def send_sums(d):
        other, to = yc_peer(d)
        send(ys.at[pair(other), :], yg.at[pair(yc), :], sent.at[15], got.at[14], to)

    each(nyc, send_sums)
    keep_y.wait()
    wait_for(count.at[0 : nyc - 1, :, 0:share], got.at[14])
    summed = mm(pair_sum(nyc), yg[...])
    for k in range(per_share):
        at_cols = slice(k * block, (k + 1) * block)
        mixed_out[:, at_cols] = (residual[k] + summed[:, at_cols])[0:2].astype(BF)
    store_mixed = pltpu.make_async_copy(mixed_out, mixed, loads.at[6])
    store_mixed.start()

    for copy in (store_c, store_n, store_m):
        copy.wait()
    wait_for(wqk.at[0 : (NY - 1) * rows, :], sent.at[0])
    wait_for(count.at[0 : nyc - 1, :, 0 : nz * lanes], sent.at[16])
    wait_for(wv.at[0 : nz - 1, 0:rows, :], sent.at[17])
    wait_for(count.at[0 : nyc - 1, :, 0 : 2 * qk], sent.at[18])
    wait_for(count.at[0 : nzc - 1, :, 0:block], sent.at[1])
    wait_for(count.at[0 : nzc - 1, :, 0:block], sent.at[2])
    wait_for(count.at[0 : nzc - 1, :, 0:128], sent.at[3])
    wait_for(wot.at[0 : (NY - 1) * rows, :], sent.at[4])
    wait_for(wd.at[0 : nz - 1, 0:rows, :], sent.at[5])
    wait_for(meta.at[0 : NY - 1], sent.at[6])
    wait_for(count.at[0 : nzc - 1, :, 0 : 2 * qk], sent.at[7])
    wait_for(count.at[0 : nzc - 1, :, 0 : 2 * qk], sent.at[8])
    wait_for(og.at[0 : n_tp * NC - 1], sent.at[9])
    wait_for(ag.at[0, 0, 0 : NY - 1], sent.at[10])
    wait_for(ag.at[0, 0 : nz - 1], sent.at[11])
    wait_for(ag.at[0], sent.at[12])
    wait_for(xg.at[0 : n_tp - 1], sent.at[13])
    wait_for(zg.at[0 : nz - 1], sent.at[14])
    wait_for(count.at[0 : nyc - 1, :, 0:share], sent.at[15])
    store_mixed.wait()


def per_device(
    tokens,
    state_c,
    state_n,
    state_m,
    mix_gain,
    w_query,
    w_key,
    w_value,
    w_input_gate,
    w_forget_gate,
    forget_bias,
    w_output,
    moe_gain,
    w_group,
    expert_ids,
    expert_weight,
    w_exp_gate,
    w_exp_up,
    w_exp_down,
    w_dense,
    w_dense_gate,
):
    n_ep, n_tp = lax.axis_size("ep"), lax.axis_size("tp")
    nz = n_ep // (NY * NC)
    width = tokens.shape[1]
    rows = w_query.shape[0]
    block = NY * NC * rows
    lanes = min(128, block)
    share = width // n_tp
    nzc, nyc = nz * NC, NY * NC
    hidden = w_exp_gate.shape[2]
    qkv = 2 * w_query.shape[1] + w_value.shape[1]
    anywhere = pl.BlockSpec(memory_space=pltpu.HBM)
    V = pltpu.VMEM

    def kernel(*refs):
        layer_kernel(n_ep, n_tp, *refs)

    in_specs = [anywhere] * 21
    out_shape = (
        jax.ShapeDtypeStruct((2, share), BF),
        jax.ShapeDtypeStruct(state_c.shape, F32),
        jax.ShapeDtypeStruct(state_n.shape, F32),
        jax.ShapeDtypeStruct(state_m.shape, F32),
    )
    scratch = [
        V((16, width), BF),
        V((block // lanes, 16, nz * lanes), BF),
        V((2 * nzc, block), BF),
        V((2 * nyc, nz * lanes), BF),
        V((2 * nzc, block), BF),
        V((16, 128), BF),
        V((NY, 2 * nzc, 128), BF),
        V((block, 2 * w_query.shape[1]), BF),
        V((nz, lanes, w_value.shape[1]), BF),
        V((block, w_output.shape[0]), BF),
        V((nz, lanes, share), BF),
        V((2 * nzc, 2 * w_query.shape[1]), BF),
        V((2 * nzc, 2 * w_query.shape[1]), BF),
        V((2 * nyc, w_value.shape[1]), BF),
        V((2 * nyc, w_value.shape[1]), BF),
        V(state_c.shape, F32),
        V(state_c.shape, F32),
        V(state_n.shape, F32),
        V(state_m.shape, F32),
        V((2, share), BF),
        V((16, w_output.shape[0]), BF),
        V((2 * nzc, w_output.shape[0]), BF),
        V((2 * nzc, block), BF),
        V((n_tp * NC, nzc, block), BF),
        V((2, nz, NY, nzc, block), BF),
        V((2 * n_ep, width), BF),
        V((2 * n_ep, 128), BF),
        V((2 * nyc, width), BF),
        V((width, hidden), BF),
        V((width, hidden), BF),
        V((hidden, width), BF),
        V((n_tp, n_ep, share), BF),
        V((n_tp, n_ep, share), BF),
        V((n_ep, share), BF),
        V((nz, nyc, share), BF),
        V((2 * nyc, share), BF),
        V((2 * nyc, share), BF),
        pltpu.SemaphoreType.DMA((32,)),
        pltpu.SemaphoreType.DMA((20,)),
        pltpu.SemaphoreType.DMA((20,)),
        pltpu.SemaphoreType.DMA((nz,)),
        pltpu.SemaphoreType.DMA((nz,)),
        pltpu.SemaphoreType.DMA((NY,)),
        pltpu.SemaphoreType.DMA((nz,)),
        V((max(nzc, nyc), 2, qkv), BF),
        V(tokens.shape, BF),
        V(state_n.shape, F32),
        V(state_m.shape, F32),
        V((1, width), F32),
        V(w_input_gate.shape[::-1], BF),
        V(w_forget_gate.shape[::-1], BF),
        V((1, forget_bias.shape[0]), F32),
        V((1, width), F32),
        V(w_group.shape[::-1], BF),
        V(expert_ids.shape, jnp.int32),
        V(expert_weight.shape, F32),
        V((width // 128, 128), BF),
    ]
    results = pl.pallas_call(
        kernel,
        name="layer",
        out_shape=out_shape,
        in_specs=in_specs,
        out_specs=(anywhere,) * 4,
        scratch_shapes=scratch,
        compiler_params=pltpu.CompilerParams(
            collective_id=0, has_side_effects=True, vmem_limit_bytes=67043328
        ),
    )(
        tokens,
        state_c,
        state_n,
        state_m,
        mix_gain.reshape(1, -1),
        w_query,
        w_key,
        w_value,
        w_input_gate.T,
        w_forget_gate.T,
        forget_bias.reshape(1, -1),
        w_output.T,
        moe_gain.reshape(1, -1),
        w_group.T,
        expert_ids,
        expert_weight,
        w_exp_gate,
        w_exp_up,
        w_exp_down,
        w_dense,
        w_dense_gate.reshape(-1, 128),
    )
    return pl.pallas_call(
        store_kernel,
        name="store",
        out_shape=out_shape,
        in_specs=[anywhere] * 4,
        out_specs=(anywhere,) * 4,
        scratch_shapes=[V(r.shape, r.dtype) for r in out_shape] + [pltpu.SemaphoreType.DMA((2, 4))],
        compiler_params=pltpu.CompilerParams(vmem_limit_bytes=67043328),
    )(*results)


def store_kernel(*refs):
    ins, outs, held, sems = refs[0:4], refs[4:8], refs[8:12], refs[12]
    order = (1, 0, 2, 3)
    for k in order:
        pltpu.make_async_copy(ins[k], held[k], sems.at[0, k]).start()
    for k in order:
        pltpu.make_async_copy(ins[k], held[k], sems.at[0, k]).wait()
        pltpu.make_async_copy(held[k], outs[k], sems.at[1, k]).start()
    for k in order:
        pltpu.make_async_copy(held[k], outs[k], sems.at[1, k]).wait()


def solution(mesh):
    placed = (
        P("ep", None),
        P("ep", "tp", None, None),
        P("ep", "tp", None),
        P("ep", "tp"),
        P(),
        P("ep", "tp"),
        P("ep", "tp"),
        P("ep", "tp"),
        P(),
        P(),
        P(),
        P("tp", "ep"),
        P(),
        P(),
        P("ep", None),
        P("ep", None),
        P("ep", None, "tp"),
        P("ep", None, "tp"),
        P("ep", "tp", None),
        P("ep", "tp"),
        P(),
    )
    return jax.shard_map(
        per_device,
        mesh=mesh,
        in_specs=placed,
        out_specs=(P("ep", "tp"), P("ep", "tp", None, None), P("ep", "tp", None), P("ep", "tp")),
        check_vma=False,
    )
```
